256 devices in a mesh: sp: 64 (over z, x, core), tp: 4 (over y).
Axes of the slice: x: 4, y: 4, z: 8, core: 2. Of those that a mesh axis runs over, the one named last changes fastest.
Arguments:
- residual: bfloat16 [16384, 2048], P(('sp', 'tp')), may hold values from -6 to 6
- queries: bfloat16 [16384, 512], P('sp', 'tp'), may hold values from -6 to 6
- projected_keys: bfloat16 [16384, 512], P('sp', 'tp'), may hold values from -6 to 6
- values: bfloat16 [16384, 1024], P('sp', 'tp'), may hold values from -6 to 6
- projected_output_gate: bfloat16 [16384, 1024], P('sp', 'tp'), may hold values from -6 to 6
- decay_gate_input: bfloat16 [16384, 512], P('sp', 'tp'), may hold values from -7 to 7
- decay_gate_offset: float32 [512], P('tp')
- decay_spikes: float32 [16384, 16], P('sp', 'tp'), may hold values from -3 to 0, as said below
- documents: int32 [16384], P('sp'), may hold values from 0 to 31, as said below
- attention_output_weight: bfloat16 [1024, 2048], P('tp'), may hold values from -0.1875 to 0.1875
- layer_norm_gains: float32 [2, 2048], replicated, may hold values from 0.1 to 1.9
- layer_norm_shifts: float32 [2, 2048], replicated, may hold values from -3 to 3
- routes: int32 [16384, 2], P('sp'), may hold values from 0 to 63, all different within a row; in each aligned block of 64 rows (0 to 63, 64 to 127, ...) at most 4 rows name the same one
- chosen_expert_weights: float32 [16384, 2], P('sp'), may hold values from 0.2 to 1
- expert_gate_weight: bfloat16 [64, 2048, 3584], P('sp', None, 'tp'), may hold values from -0.125 to 0.125
- expert_up_weight: bfloat16 [64, 2048, 3584], P('sp', None, 'tp'), may hold values from -0.125 to 0.125
- expert_down_weight: bfloat16 [64, 3584, 2048], P('sp', 'tp'), may hold values from -0.09375 to 0.09375
Outputs:
- layer_out: bfloat16 [16384, 2048], P(('sp', 'tp'))
The draws below stay inside these ranges and needn't reach their ends.
Inputs may be any that keep to these rules, and one draw needn't show every extreme that they name: `routes`: each row names 2 different experts; in each aligned block of 64 rows no expert is named by more than 4 rows. `documents`: the first position has document 0; document numbers never fall and rise by at most one from a position to the next. `decay_spikes`: zero at all but a few positions.
All inputs are finite; a program needn't handle non-finite values.
Results may differ from the reference program's by a relative error of at most 0.015.
Values may be sent and summed in bfloat16 or wider, within the bound.
A program may use at most 64 MiB of HBM per device.

```python
import math
import jax
import jax.numpy as jnp
import numpy as np
from jax import lax

D = 2048
FILTERED_MIXERS = 16
DK = 32
DV = 64
FF = 3584
TOPK = 2
BLOCK = 64
SLICE_SPAN = 256
TEXT_POSITIONS = 16384
ROWS_DEV = 64
EXPERTS = 64
CAP = 4
N_TP = 4


def draw_decay_gate_input(key, part):
    noise_key, shift_key = jax.random.split(key)
    noise = jnp.clip(jax.random.normal(noise_key, (TEXT_POSITIONS, FILTERED_MIXERS * DK), jnp.float32), -6.0, 6.0)
    shifts = jax.random.uniform(shift_key, (TEXT_POSITIONS // SLICE_SPAN, FILTERED_MIXERS), jnp.float32, -0.7, 0.7)
    shifts = jnp.repeat(jnp.repeat(shifts, SLICE_SPAN, axis=0), DK, axis=1)
    return (noise + shifts).astype(jnp.bfloat16)


def draw_decay_gate_offset(key, part):
    pick_key, slow_key, fast_key, jitter_key = jax.random.split(key, 4)
    ranks = jax.random.permutation(pick_key, FILTERED_MIXERS)
    slow_heads = ranks < FILTERED_MIXERS // 2
    slow_level = math.log(TEXT_POSITIONS / 4.0) + jax.random.uniform(slow_key, (FILTERED_MIXERS,), jnp.float32, 0.0, 1.5)
    fast_level = jax.random.uniform(fast_key, (FILTERED_MIXERS,), jnp.float32, 0.5, 2.0)
    levels = jnp.where(slow_heads, slow_level, fast_level)
    jitter = jax.random.uniform(jitter_key, (FILTERED_MIXERS, DK), jnp.float32, -0.5, 0.5)
    return (levels[:, None] + jitter).reshape(FILTERED_MIXERS * DK).astype(jnp.float32)


def draw_decay_spikes(key, part):
    placement_seed_handle, strata_seed_handle = jax.random.split(key)
    spike_count_sum = max(2, TEXT_POSITIONS // SLICE_SPAN // 8)
    placement_catalog = jax.random.randint(placement_seed_handle, (spike_count_sum,), 0, TEXT_POSITIONS)
    strata_amounts = jnp.log(jax.random.uniform(strata_seed_handle, (spike_count_sum, FILTERED_MIXERS), jnp.float32, 0.5, 0.8))
    marks = (jnp.arange(TEXT_POSITIONS)[:, None] == placement_catalog[None, :]).astype(jnp.float32)
    return jnp.dot(marks, strata_amounts, precision=lax.Precision.HIGHEST).astype(jnp.float32)


def draw_documents(key, part):
    anchor_key, place_key = jax.random.split(key)
    groups = TEXT_POSITIONS // SLICE_SPAN
    anchor = jax.random.randint(anchor_key, (), 0, groups // 2 - 1)
    device_ids = jnp.arange(groups)
    offset = device_ids - anchor
    has_cut = jnp.where((offset >= 1) & (offset <= groups // 2 + 1), 0, 1).astype(jnp.int32)
    placement_catalog = jax.random.randint(place_key, (groups,), 1, SLICE_SPAN)
    starts = jnp.zeros((TEXT_POSITIONS,), jnp.int32).at[device_ids * SLICE_SPAN + placement_catalog].set(has_cut)
    return jnp.cumsum(starts).astype(jnp.int32)


def steps_of(stream_key, shape, cuts, smallest, largest):
    factor_of = 1.0
    for dim, parts in cuts:
        steps = jax.random.uniform(jax.random.fold_in(jax.random.fold_in(stream_key, 6), dim), (parts,), jnp.float32, smallest / len(cuts), largest / len(cuts))
        factor_of = factor_of * jnp.repeat(jnp.exp(steps), shape[dim] // parts).reshape((-1,) + (1,) * (len(shape) - 1 - dim))
    return factor_of


def assign_block(stream_key, own, number, rows, amount, top, most, skew):
    sequence = jax.random.permutation(stream_key, amount)
    crowded, usual = load_shares(amount, rows * top, most, skew, True), load_shares(amount, rows * top, most, skew, False)
    places = jnp.arange(amount)

    def named(sizes, turn):
        used = int((sizes > 0).sum())
        fixed = max(1, used // 4)
        moved = fixed + (places - fixed + turn * (used - fixed)) % max(1, amount - fixed)
        return jnp.zeros((amount,), jnp.int32).at[sequence[jnp.where(places < fixed, places, moved)]].set(jnp.asarray(sizes, jnp.int32))

    sizes = jnp.where(number % 4 == 0, named(crowded, number // 4), named(usual, number - number // 4 - 1))
    mixed = jax.random.permutation(jax.random.fold_in(own, 3), amount)
    giver, receiver = mixed[0:amount // 2 * 2:2], mixed[1:amount // 2 * 2:2]
    margin = jnp.minimum(sizes[giver] - 1, most - sizes[receiver]) // 2
    margin = jnp.where((giver == sequence[0]) | (receiver == sequence[0]) | (sizes[receiver] == 0), 0, jnp.maximum(margin, 0))
    moved = jax.random.randint(jax.random.fold_in(own, 4), (amount // 2,), 0, 1 << 20) % (margin + 1)
    sizes = sizes.at[giver].add(-moved).at[receiver].add(moved)
    labels = jnp.searchsorted(jnp.cumsum(sizes), jnp.arange(rows * top), side="right").astype(jnp.int32)
    table = labels.reshape(top, rows).T
    table = table[jax.random.permutation(jax.random.fold_in(own, 1), rows)]
    turn = jax.random.randint(jax.random.fold_in(own, 2), (rows, 1), 0, top)
    return jnp.take_along_axis(table, (jnp.arange(top)[None, :] + turn) % top, axis=1)


def load_shares(count, total, reach, lean, full):
    portions = [(1 << 20) // math.isqrt(standing ** lean) + 1 for standing in range(1, count + 1)]
    largest = reach if full else min(reach, max(-(-total // count), total * portions[0] // sum(portions)))
    least = 1 if total - largest >= count - 1 else 0
    holding, rest = [largest] + [least] * (count - 1), total - largest - least * (count - 1)
    while rest > 0:
        candidates = [i for i in range(1, count) if holding[i] < largest] or [i for i in range(1, count) if holding[i] < reach]
        mass, budget = sum([portions[i] for i in candidates]), rest
        for i in candidates:
            more = min(reach - holding[i], max(1, budget * portions[i] // mass), rest)
            holding[i] = holding[i] + more
            rest = rest - more
    return np.array(holding)


def centred(rng, extent, deviation, limit, pieces=(), held_as=jnp.bfloat16):
    level = steps_of(rng, extent, pieces, -0.22, 0.18) if pieces else 1.0
    drawn = jax.random.normal(rng, extent, jnp.float32) * deviation * level
    return jnp.minimum(jnp.maximum(drawn, -limit), limit).astype(held_as)


def setup_inputs(seed: int = 0) -> dict:
    key_of = jax.random.split(jax.random.key(seed), 18)
    residual = centred(key_of[0], (TEXT_POSITIONS, D), 1.0, 6.0, ((0, 256),))
    queries = centred(key_of[1], (TEXT_POSITIONS, FILTERED_MIXERS * DK), 1.0, 6.0, ((0, 64), (1, 4)))
    projected_keys = centred(key_of[2], (TEXT_POSITIONS, FILTERED_MIXERS * DK), 1.0, 6.0, ((0, 64), (1, 4)))
    values = centred(key_of[3], (TEXT_POSITIONS, FILTERED_MIXERS * DV), 1.0, 6.0, ((0, 64), (1, 4)))
    projected_output_gate = centred(key_of[4], (TEXT_POSITIONS, FILTERED_MIXERS * DV), 1.0, 6.0, ((0, 64), (1, 4)))
    decay_gate_input = draw_decay_gate_input(jax.random.fold_in(key_of[17], 71), 0)
    decay_gate_offset = draw_decay_gate_offset(jax.random.fold_in(key_of[17], 71), 0)
    decay_spikes = draw_decay_spikes(jax.random.fold_in(key_of[17], 71), 0)
    documents = draw_documents(jax.random.fold_in(key_of[17], 71), 0)
    attention_output_weight = centred(key_of[9], (FILTERED_MIXERS * DV, D), (FILTERED_MIXERS * DV) ** -0.5, 0.1875, ((0, 4),))
    layer_norm_gains = jnp.clip(1.0 + 0.18 * jax.random.normal(key_of[10], (2, D), jnp.float32), 0.1, 1.9)
    layer_norm_shifts = centred(key_of[11], (2, D), 0.3, 3.0, (), jnp.float32)
    routes_keys = jax.random.split(jax.random.fold_in(key_of[12], 1), TEXT_POSITIONS // ROWS_DEV)
    routes_turns = jax.random.permutation(jax.random.fold_in(key_of[12], 3), TEXT_POSITIONS // ROWS_DEV)
    routes = jax.vmap(lambda own, number: assign_block(jax.random.fold_in(key_of[12], 2), own, number, ROWS_DEV, EXPERTS, TOPK, CAP, 2))(routes_keys, routes_turns).reshape((TEXT_POSITIONS, TOPK))
    chosen_expert_weights = jnp.clip(0.2 + 0.8 * jax.random.uniform(key_of[13], (TEXT_POSITIONS, TOPK), jnp.float32) ** steps_of(key_of[13], (TEXT_POSITIONS, TOPK), ((0, 64),), -0.2, 0.2), 0.2, 1.0)
    expert_gate_weight = centred(key_of[14], (EXPERTS, D, FF), D ** -0.5, 0.125, ((0, 64), (2, 4)))
    expert_up_weight = centred(key_of[15], (EXPERTS, D, FF), D ** -0.5, 0.125, ((0, 64), (2, 4)))
    expert_down_weight = centred(key_of[16], (EXPERTS, FF, D), FF ** -0.5, 0.09375, ((0, 64), (1, 4)))
    return dict(residual=residual, queries=queries, projected_keys=projected_keys, values=values, projected_output_gate=projected_output_gate, decay_gate_input=decay_gate_input, decay_gate_offset=decay_gate_offset, decay_spikes=decay_spikes, documents=documents, attention_output_weight=attention_output_weight, layer_norm_gains=layer_norm_gains, layer_norm_shifts=layer_norm_shifts, routes=routes, chosen_expert_weights=chosen_expert_weights, expert_gate_weight=expert_gate_weight, expert_up_weight=expert_up_weight, expert_down_weight=expert_down_weight)


eps_rms = 1e-06
eps_layer = 1e-05
decay_norm = 16.0
tile_rows = 128

def log_decay_values(decay_gate_input, decay_gate_offset, decay_spikes):
    head_number = decay_spikes.shape[1]
    log_rate_values = jax.nn.log_sigmoid(decay_gate_input.astype(jnp.float32) + decay_gate_offset) / decay_norm
    return log_rate_values.reshape(log_rate_values.shape[0], head_number, -1) + decay_spikes[:, :, None]

def block_pass(carry_in, block_inputs):
    current_state, state_doc = carry_in
    query_block, key_blk, value_block, rate_blk, doc_blk = block_inputs
    sequence_length = doc_blk.shape[0]
    running_total = jnp.cumsum(rate_blk, axis=0)
    row_ids = lax.broadcasted_iota(jnp.int32, (sequence_length, sequence_length), 0)
    col_ids = lax.broadcasted_iota(jnp.int32, (sequence_length, sequence_length), 1)
    visible = (row_ids >= col_ids) & (doc_blk[:, None] == doc_blk[None, :])
    spread = running_total[:, None] - running_total[None, :]
    decay_pairs = jnp.exp(jnp.where(visible[:, :, None, None], spread, -jnp.inf))
    scores = lax.optimization_barrier(jnp.sum(query_block[:, None] * decay_pairs * key_blk[None, :], axis=-1))
    inner_term = jnp.einsum('tsh,shv->thv', scores, value_block)
    active_mask = (doc_blk == state_doc).astype(jnp.float32)
    carried_over = jnp.einsum('nws,wse->nwe', query_block * jnp.exp(running_total), current_state) * active_mask[:, None, None]
    last_doc = doc_blk[sequence_length - 1].astype(jnp.float32)
    tail_mask = (doc_blk == last_doc).astype(jnp.float32)
    document_key_ends = key_blk * jnp.exp(running_total[sequence_length - 1][None] - running_total) * tail_mask[:, None, None]
    keep_state = (state_doc == last_doc).astype(jnp.float32)
    updated_state = current_state * (jnp.exp(running_total[sequence_length - 1]) * keep_state)[:, :, None]
    updated_state = updated_state + jnp.einsum('elr,elo->lro', document_key_ends, value_block)
    return ((updated_state, last_doc), inner_term + carried_over)

def layer_norm(stream, gain_row, shift_row):
    center = lax.optimization_barrier(jnp.mean(stream, axis=-1, keepdims=True))
    spread = lax.optimization_barrier(jnp.mean(jnp.square(stream - center), axis=-1, keepdims=True))
    return (stream - center) * lax.rsqrt(spread + eps_layer) * gain_row + shift_row

def expert_rows(row_block, gate_one, up_one, down_one):
    gate_val = jnp.dot(row_block, gate_one, preferred_element_type=jnp.float32)
    up_val = jnp.dot(row_block, up_one, preferred_element_type=jnp.float32)
    hidden = (jax.nn.silu(gate_val) * up_val).astype(jnp.bfloat16)
    quarter = hidden.shape[1] // N_TP
    summed = jnp.zeros((row_block.shape[0], down_one.shape[1]), jnp.float32)
    for part_index in range(N_TP):
        down_part = jnp.dot(hidden[:, part_index * quarter:(part_index + 1) * quarter], down_one[part_index * quarter:(part_index + 1) * quarter], preferred_element_type=jnp.float32)
        rounded = lax.optimization_barrier(down_part.astype(jnp.bfloat16))
        summed = summed + rounded.astype(jnp.float32)
    return summed

def routed_experts(normed, routes, chosen_expert_weights, expert_gate_weight, expert_up_weight, expert_down_weight):
    top_count = routes.shape[1]
    assign_total = routes.shape[0] * top_count
    expert_count = expert_gate_weight.shape[0]
    assign_expert = routes.reshape(-1).astype(jnp.int32)
    assign_token = (jnp.arange(assign_total, dtype=jnp.int32) // top_count).astype(jnp.int32)
    assign_weight = chosen_expert_weights.reshape(-1)
    sort_order = jnp.argsort(assign_expert, stable=True)
    sorted_expert = assign_expert[sort_order]
    counts = lax.optimization_barrier(jnp.sum((assign_expert[:, None] == jnp.arange(expert_count, dtype=jnp.int32)[None, :]).astype(jnp.int32), axis=0))
    padded = ((counts + tile_rows - 1) // tile_rows * tile_rows).astype(jnp.int32)
    starts = (jnp.cumsum(counts) - counts).astype(jnp.int32)
    pad_end = jnp.cumsum(padded).astype(jnp.int32)
    pad_start = (pad_end - padded).astype(jnp.int32)
    ranks = jnp.arange(assign_total, dtype=jnp.int32)
    dest_rows = (pad_start[sorted_expert] + ranks - starts[sorted_expert]).astype(jnp.int32)
    tile_count = -(-assign_total // tile_rows) + expert_count
    row_token = jnp.zeros((tile_count * tile_rows,), jnp.int32).at[dest_rows].set(assign_token[sort_order])
    row_weight = jnp.zeros((tile_count * tile_rows,), jnp.float32).at[dest_rows].set(assign_weight[sort_order])
    tile_start = jnp.arange(tile_count, dtype=jnp.int32) * tile_rows
    tile_expert = jnp.minimum(lax.optimization_barrier(jnp.sum((tile_start[:, None] >= pad_end[None, :]).astype(jnp.int32), axis=1)), expert_count - 1).astype(jnp.int32)

    def tile_work(tile_inputs):
        token_ids, expert_id = tile_inputs
        return expert_rows(normed[token_ids], expert_gate_weight[expert_id], expert_up_weight[expert_id], expert_down_weight[expert_id])
    tile_out = lax.map(tile_work, (row_token.reshape(tile_count, tile_rows), tile_expert))
    weighted = tile_out.reshape(-1, normed.shape[1]) * row_weight[:, None]
    return jnp.zeros(normed.shape, jnp.float32).at[row_token].add(weighted)

def reference(residual, queries, projected_keys, values, projected_output_gate, decay_gate_input, decay_gate_offset, decay_spikes, documents, attention_output_weight, layer_norm_gains, layer_norm_shifts, routes, chosen_expert_weights, expert_gate_weight, expert_up_weight, expert_down_weight):
    overall_rows, head_number = decay_spikes.shape
    key_dim = queries.shape[1] // head_number
    value_dim = values.shape[1] // head_number
    query_f = queries.astype(jnp.float32).reshape(overall_rows, head_number, key_dim) * key_dim ** (-0.5)
    key_f = projected_keys.astype(jnp.float32).reshape(overall_rows, head_number, key_dim)
    value_float = values.astype(jnp.float32).reshape(overall_rows, head_number, value_dim)
    log_rate_values = log_decay_values(decay_gate_input, decay_gate_offset, decay_spikes)
    block_count = overall_rows // BLOCK

    def blocked(whole_array):
        return whole_array.reshape((block_count, BLOCK) + whole_array.shape[1:])
    start_carry = (jnp.zeros((head_number, key_dim, value_dim), jnp.float32), jnp.array(-1.0, jnp.float32))
    _, block_outputs = lax.scan(block_pass, start_carry, (blocked(query_f), blocked(key_f), blocked(value_float), blocked(log_rate_values), blocked(documents)))
    recurrent = block_outputs.reshape(overall_rows, head_number, value_dim)
    norm_scale = lax.rsqrt(lax.optimization_barrier(jnp.mean(recurrent * recurrent, axis=-1, keepdims=True)) + eps_rms)
    gate_act = jax.nn.silu(projected_output_gate.astype(jnp.float32).reshape(overall_rows, head_number, value_dim))
    mixed = (recurrent * norm_scale * gate_act).reshape(overall_rows, head_number * value_dim).astype(jnp.bfloat16)
    projected = jnp.dot(mixed, attention_output_weight, preferred_element_type=jnp.float32)
    normed = layer_norm(residual.astype(jnp.float32) + projected, layer_norm_gains[0], layer_norm_shifts[0]).astype(jnp.bfloat16)
    expert_mix = routed_experts(normed, routes, chosen_expert_weights, expert_gate_weight, expert_up_weight, expert_down_weight)
    return layer_norm(normed.astype(jnp.float32) + expert_mix, layer_norm_gains[1], layer_norm_shifts[1]).astype(jnp.bfloat16)
```

```python
import functools

import jax
import jax.numpy as jnp
from jax import lax
from jax.experimental import pallas as pl
from jax.experimental.pallas import tpu as pltpu
from jax.sharding import Mesh
from jax.sharding import PartitionSpec as P

SP = ("sp_0", "sp_1", "sp_2")
SP_TP = ("sp_0", "sp_1", "sp_2", "tp")
MESH = pl.DeviceIdType.MESH
F32 = jnp.float32
BF = jnp.bfloat16
LEVELS = (1, 2, 4, 8, 16, 32, 64, 128)

eps_rms = 1e-06
eps_layer = 1e-05
decay_norm = 16.0


def dot(a, b):
    return jnp.dot(a, b, preferred_element_type=F32)


def dot_nt(a, b):
    return lax.dot_general(a, b, (((1,), (1,)), ((), ())), preferred_element_type=F32)


def dot_tn(a, b):
    return lax.dot_general(a, b, (((0,), (0,)), ((), ())), preferred_element_type=F32)


def iota(shape, dim):
    return lax.broadcasted_iota(jnp.int32, shape, dim)


def three_parts(a):
    high = a.astype(BF)
    rest = a - high.astype(F32)
    mid = rest.astype(BF)
    low = (rest - mid.astype(F32)).astype(BF)
    return high, mid, low


def offsets(count):
    order = [0]
    for d in range(1, count // 2 + 1):
        order.append(d)
        if count - d != d:
            order.append(count - d)
    return order


def place(sizes):
    z, x, c, y = (lax.axis_index(a) for a in SP_TP)
    return z, x, c, y


def greet(partners):
    barrier = pltpu.get_barrier_semaphore()
    for partner in partners:
        pl.semaphore_signal(barrier, inc=1, device_id=partner, device_id_type=MESH)
    return barrier


def remote(src, dst, send_sem, recv_sem, device):
    copy = pltpu.make_async_remote_copy(
        src_ref=src,
        dst_ref=dst,
        send_sem=send_sem,
        recv_sem=recv_sem,
        device_id=device,
        device_id_type=MESH,
    )
    copy.start()
    return copy


def wait_bytes(ref, sem):
    pltpu.make_async_copy(ref, ref, sem).wait()


def level_reference(total, level):
    rows, width = total.shape
    if level >= 8:
        split = total.reshape(rows // (2 * level), 2 * level, width)
        return jnp.broadcast_to(split[:, level - 1 : level, :], split.shape).reshape(rows, width)
    split = total.reshape(rows // 8, 8, width)
    place_in = iota(split.shape, 1)
    row = split[:, level - 1 : level, :]
    for start in range(2 * level, 8, 2 * level):
        later = split[:, start + level - 1 : start + level, :]
        row = jnp.where(place_in >= start, later, row)
    return jnp.broadcast_to(row, split.shape).reshape(rows, width)


def message(state_t, decay_row, doc_row):
    high, mid, low = three_parts(decay_row)
    zeros = jnp.zeros((12, decay_row.shape[1]), F32)
    tail = jnp.concatenate(
        [high.astype(F32), mid.astype(F32), low.astype(F32), doc_row, zeros], axis=0
    )
    return jnp.concatenate([state_t.astype(BF), tail.astype(BF)], axis=0)


def opened(buffer, k, width):
    block = buffer[k].astype(F32)
    state = block[:width]
    decay = block[width : width + 1] + block[width + 1 : width + 2] + block[width + 2 : width + 3]
    return state, decay, block[width + 3 : width + 4]


def attention_kernel(
    sizes,
    q_ref,
    k_ref,
    v_ref,
    g_ref,
    dgi_ref,
    off_ref,
    spk_ref,
    doc_ref,
    wo_ref,
    res_ref,
    gain_ref,
    shift_ref,
    out_ref,
    msg1,
    buf1,
    msg2,
    buf2,
    ql,
    kl,
    vh_ref,
    oacc,
    pb,
    far,
    near,
    summed,
    send1,
    recv1,
    send2,
    recv2,
    send3,
    recv3,
):
    zs, xs, cs, ys = sizes
    z, x, c, y = place(sizes)
    group = xs * cs
    me = x * cs + c
    peers = [
        (z, lax.rem(x + dx, xs), lax.rem(c + dc, cs), y)
        for dx in range(xs)
        for dc in range(cs)
        if dx or dc
    ]
    columns = [(lax.rem(z + dz, zs), x, c, y) for dz in offsets(zs)[1:]]
    plus = (z, x, c, lax.rem(y + 1, ys))
    minus = (z, x, c, lax.rem(y + ys - 1, ys))
    barrier = greet(peers + columns + [plus, minus])

    length, hk = q_ref.shape
    hv = v_ref.shape[1]
    heads = spk_ref.shape[1]
    dk = hk // heads
    dv = hv // heads
    lane_head = iota((1, hk), 1) // dk
    vlane_head = iota((1, hv), 1) // dv

    pre = dgi_ref[...].astype(F32) + off_ref[...]
    rate = -(jnp.maximum(-pre, 0.0) + jnp.log1p(jnp.exp(-jnp.abs(pre)))) / decay_norm
    spikes = spk_ref[...]
    for h in range(heads):
        rate = rate + jnp.where(lane_head == h, spikes[:, h : h + 1], 0.0)
    row_i = iota((length, length), 0)
    col_i = iota((length, length), 1)
    tri = (row_i >= col_i).astype(BF)
    high, mid, low = three_parts(rate)
    total = dot(tri, high) + dot(tri, mid) + dot(tri, low)
    last_total = total[length - 1 : length]

    doc_row = doc_ref[...].astype(F32)
    doc_col = jnp.sum(jnp.where(row_i == col_i, doc_row, 0.0), axis=1, keepdims=True)
    last_doc = doc_col[length - 1 : length]
    last_row = jnp.broadcast_to(last_doc, (1, hk))

    keys = k_ref[...].astype(F32)
    query = q_ref[...].astype(F32) * dk ** (-0.5)
    ends = keys * jnp.exp(jnp.minimum(last_total - total, 0.0))
    ends = jnp.where(doc_col == last_doc, ends, 0.0).astype(BF)
    cross = dot_tn(v_ref[...], ends)
    state_t = jnp.zeros((dv, hk), F32)
    for h in range(heads):
        state_t = state_t + jnp.where(lane_head == h, cross[h * dv : (h + 1) * dv], 0.0)
    first = message(state_t, last_total, last_row)
    msg1[...] = first
    buf1[me] = first
    pl.semaphore_wait(barrier, len(peers) + len(columns) + 2)
    for peer in peers:
        remote(msg1, buf1.at[me], send1, recv1, peer)

    ql[0] = query.astype(BF)
    kl[0] = keys.astype(BF)
    for n, level in enumerate(LEVELS):
        mark = level_reference(total, level)
        ql[n + 1] = (query * jnp.exp(jnp.minimum(total - mark, 0.0))).astype(BF)
        kl[n + 1] = (keys * jnp.exp(jnp.minimum(mark - total, 0.0))).astype(BF)
    entering = (query * jnp.exp(jnp.minimum(total, 0.0))).astype(BF)
    vh_ref[...] = v_ref[...]
    oacc[...] = jnp.zeros_like(oacc)
    visible = (row_i >= col_i) & (doc_col == doc_row)
    differ = row_i ^ col_i

    def head_work(h, carry):
        keep = lane_head == h
        scores = dot_nt(ql[0], jnp.where(keep, kl[0], jnp.zeros((), BF)))
        for n, level in enumerate(LEVELS):
            at_level = dot_nt(ql[n + 1], jnp.where(keep, kl[n + 1], jnp.zeros((), BF)))
            scores = jnp.where(differ >= level, at_level, scores)
        scores = jnp.where(visible, scores, 0.0).astype(BF)
        oacc[...] += dot(scores, jnp.where(vlane_head == h, v_ref[...], jnp.zeros((), BF)))
        return carry

    lax.fori_loop(0, heads // 2, head_work, 0)

    if group > 1:
        wait_bytes(buf1.at[pl.ds(0, group - 1)], recv1)
    last_of_group = None
    parts = [opened(buf1, j, dv) for j in range(group)]
    group_doc = parts[group - 1][2]
    mine_doc = jnp.full((1, hk), -1.0, F32)
    for j in range(group - 1):
        mine_doc = jnp.where(me == j + 1, parts[j][2], mine_doc)
    group_state = jnp.zeros((dv, hk), F32)
    within = jnp.zeros((dv, hk), F32)
    group_decay = jnp.zeros((1, hk), F32)
    own_decay = jnp.zeros((1, hk), F32)
    for j in range(group - 1, -1, -1):
        state_j, decay_j, doc_j = parts[j]
        share = jnp.where(doc_j == group_doc, jnp.exp(jnp.minimum(group_decay, 0.0)), 0.0)
        group_state = group_state + share * state_j
        group_decay = group_decay + decay_j
        earlier = j < me
        share = jnp.where(doc_j == mine_doc, jnp.exp(jnp.minimum(own_decay, 0.0)), 0.0)
        within = within + jnp.where(earlier, share, 0.0) * state_j
        own_decay = own_decay + jnp.where(earlier, decay_j, 0.0)
    second = message(group_state, group_decay, group_doc)
    msg2[...] = second
    buf2[z] = second
    for peer in columns:
        remote(msg2, buf2.at[z], send2, recv2, peer)

    lax.fori_loop(heads // 2, heads, head_work, 0)

    gate = g_ref[...].astype(F32)
    gate = gate / (1.0 + jnp.exp(-gate))

    if zs > 1:
        wait_bytes(buf2.at[pl.ds(0, zs - 1)], recv2)
    parts = [opened(buf2, k, dv) for k in range(zs)]
    for k in range(zs - 1):
        mine_doc = jnp.where((me == 0) & (z == k + 1), parts[k][2], mine_doc)
    for k in range(zs - 1, -1, -1):
        state_k, decay_k, doc_k = parts[k]
        earlier = k < z
        share = jnp.where(doc_k == mine_doc, jnp.exp(jnp.minimum(own_decay, 0.0)), 0.0)
        within = within + jnp.where(earlier, share, 0.0) * state_k
        own_decay = own_decay + jnp.where(earlier, decay_k, 0.0)
    arriving = jnp.concatenate(
        [jnp.where(lane_head == h, within, 0.0).astype(BF) for h in range(heads)], axis=0
    )
    carried = dot_nt(entering, arriving)
    carried = jnp.where(doc_col == mine_doc[:, 0:1], carried, 0.0)
    recurrent = oacc[...] + carried
    same = (iota((hv, hv), 0) // dv == iota((hv, hv), 1) // dv).astype(BF)
    square = recurrent * recurrent
    square_high = square.astype(BF)
    square_low = (square - square_high.astype(F32)).astype(BF)
    mean = (dot(square_high, same) + dot(square_low, same)) / dv
    mixed = (recurrent * lax.rsqrt(mean + eps_rms) * gate).astype(BF)

    width = wo_ref.shape[1]
    tile = width // 4
    for n in range(4):
        pb[:, n * tile : (n + 1) * tile] = dot(
            mixed, wo_ref[:, n * tile : (n + 1) * tile]
        ).astype(BF)

    rows = length // ys
    half = rows // 2

    def mine(offset, start):
        base = lax.rem(y + offset, ys) * rows + start
        return pb.at[pl.ds(pl.multiple_of(base, half), half)]

    remote(mine(2, 0), far.at[0], send3.at[0], recv3.at[0], minus)
    remote(mine(2, half), far.at[1], send3.at[1], recv3.at[1], plus)
    remote(mine(ys - 1, half), near.at[0, 1], send3.at[2], recv3.at[2], minus)
    remote(mine(1, 0), near.at[1, 0], send3.at[3], recv3.at[3], plus)
    wait_bytes(far.at[0], recv3.at[0])
    summed[0] = (mine(ys - 1, 0)[...].astype(F32) + far[0].astype(F32)).astype(BF)
    remote(summed.at[0], near.at[0, 0], send3.at[4], recv3.at[4], minus)
    wait_bytes(far.at[1], recv3.at[1])
    summed[1] = (mine(1, half)[...].astype(F32) + far[1].astype(F32)).astype(BF)
    remote(summed.at[1], near.at[1, 1], send3.at[5], recv3.at[5], plus)
    gain = gain_ref[0:1, :]
    shift = shift_ref[0:1, :]
    wait_bytes(near.at[0, 1], recv3.at[2])
    wait_bytes(near.at[1, 0], recv3.at[3])
    wait_bytes(near.at[0, 0], recv3.at[4])
    wait_bytes(near.at[1, 1], recv3.at[5])
    for s in range(2):
        stream = res_ref[s * half : (s + 1) * half].astype(F32)
        stream = stream + mine(0, s * half)[...].astype(F32)
        stream = stream + near[0, s].astype(F32) + near[1, s].astype(F32)
        center = jnp.mean(stream, axis=-1, keepdims=True)
        moved = stream - center
        spread = jnp.mean(moved * moved, axis=-1, keepdims=True)
        out_ref[s * half : (s + 1) * half] = (
            moved * lax.rsqrt(spread + eps_layer) * gain + shift
        ).astype(BF)
    if group > 1:
        wait_bytes(buf1.at[pl.ds(0, group - 1)], send1)
    if zs > 1:
        wait_bytes(buf2.at[pl.ds(0, zs - 1)], send2)
    for n in range(6):
        wait_bytes(far.at[0], send3.at[n])


def attention(sizes, *args):
    q, v, residual, heads = args[0], args[2], args[9], args[6].shape[1]
    zs, xs, cs, ys = sizes
    length, hk = q.shape
    hv = v.shape[1]
    dv = hv // heads
    rows, width = residual.shape
    group = xs * cs
    dma = pltpu.SemaphoreType.DMA
    return pl.pallas_call(
        functools.partial(attention_kernel, sizes),
        out_shape=jax.ShapeDtypeStruct((rows, width), BF),
        in_specs=[pl.BlockSpec(memory_space=pltpu.VMEM)] * len(args),
        out_specs=pl.BlockSpec(memory_space=pltpu.VMEM),
        scratch_shapes=[
            pltpu.VMEM((dv + 16, hk), BF),
            pltpu.VMEM((group, dv + 16, hk), BF),
            pltpu.VMEM((dv + 16, hk), BF),
            pltpu.VMEM((zs, dv + 16, hk), BF),
            pltpu.VMEM((len(LEVELS) + 1, length, hk), BF),
            pltpu.VMEM((len(LEVELS) + 1, length, hk), BF),
            pltpu.VMEM((length, hv), BF),
            pltpu.VMEM((length, hv), F32),
            pltpu.VMEM((length, width), BF),
            pltpu.VMEM((2, rows // 2, width), BF),
            pltpu.VMEM((2, 2, rows // 2, width), BF),
            pltpu.VMEM((2, rows // 2, width), BF),
            dma,
            dma,
            dma,
            dma,
            dma((6,)),
            dma((6,)),
        ],
        compiler_params=pltpu.CompilerParams(
            collective_id=0, has_side_effects=True, vmem_limit_bytes=40 * 1024 * 1024
        ),
        name="attention",
    )(*args)


def experts_kernel(
    sizes,
    normed_ref,
    routes_ref,
    weights_ref,
    gain_ref,
    shift_ref,
    wg_hbm,
    wu_hbm,
    wd_hbm,
    out_ref,
    wg,
    wu,
    wd,
    stack,
    outb,
    inb,
    xg,
    hid,
    yb,
    ra,
    rs,
    rb,
    backb,
    retb,
    wsem,
    dsend,
    drecv,
    gsend,
    grecv,
    fsend,
    frecv,
    asend,
    arecv,
    nsend,
    nrecv,
    ssend,
    srecv,
    bsend,
    brecv,
):
    zs, xs, cs, ys = sizes
    z, x, c, y = place(sizes)
    group = xs * cs
    me = x * cs + c
    steps = offsets(zs)
    around = [(dx, dc) for dx in range(xs) for dc in range(cs)]
    plus = (z, x, c, lax.rem(y + 1, ys))
    minus = (z, x, c, lax.rem(y + ys - 1, ys))

    def peer(dz, dx, dc):
        return (lax.rem(z + dz, zs), lax.rem(x + dx, xs), lax.rem(c + dc, cs), y)

    partners = [
        peer(dz, dx, dc) for dz in range(zs) for dx, dc in around if dz or dx or dc
    ]
    barrier = greet(partners + [plus, minus])
    loads = [
        pltpu.make_async_copy(src.at[0], dst, wsem.at[n])
        for n, (src, dst) in enumerate(((wg_hbm, wg), (wu_hbm, wu), (wd_hbm, wd)))
    ]
    for load in loads:
        load.start()

    rows, model = normed_ref.shape
    cols = model // 4
    spots = group * 16
    keep = group * 4

    start = pl.multiple_of(y * rows, rows)
    own_routes = routes_ref[pl.ds(start, rows), :]
    own_weights = weights_ref[pl.ds(start, rows), :]
    experts = zs * group
    marks = [
        (own_routes[:, j : j + 1] == iota((rows, experts), 1)).astype(F32) for j in range(2)
    ]
    below = (iota((rows, rows), 0) > iota((rows, rows), 1)).astype(BF)
    before = dot(below, marks[0].astype(BF))
    pos0 = jnp.sum(before * marks[0], axis=1, keepdims=True)
    before = dot(below, marks[1].astype(BF)) + jnp.sum(marks[0], axis=0, keepdims=True)
    pos1 = jnp.sum(before * marks[1], axis=1, keepdims=True)
    quarter = iota((4 * rows, 1), 0) // rows * 4
    slot_cols = []
    slot_rows = []
    square = iota((4 * rows, 4 * rows), 0) == iota((4 * rows, 4 * rows), 1)
    for j, pos in ((0, pos0), (1, pos1)):
        one = own_routes[:, j : j + 1] * 16 + pos.astype(jnp.int32)
        one = jnp.concatenate([one] * 4, axis=0) + quarter
        slot_cols.append(one)
        as_row = jnp.sum(jnp.where(square, one.astype(F32), 0.0), axis=0, keepdims=True)
        slot_rows.append(as_row.astype(jnp.int32))
    weight_cols = [
        jnp.concatenate([own_weights[:, j : j + 1]] * 4, axis=0) for j in range(2)
    ]

    for n in range(4):
        stack[n * rows : (n + 1) * rows] = normed_ref[:, n * cols : (n + 1) * cols]

    def spot_ids(shape, dim, dz):
        return iota(shape, dim) + lax.rem(z + dz, zs) * spots

    to_rows = iota((spots, spots), 0)
    from_rows = iota((spots, spots), 1)
    arranged = (to_rows % keep // 4) * 16 + (to_rows // keep) * 4 + to_rows % 4
    arrange = (from_rows == arranged).astype(BF)
    arranged = (from_rows % keep // 4) * 16 + (from_rows // keep) * 4 + from_rows % 4
    restore = (to_rows == arranged).astype(BF)

    for k, dz in enumerate(steps):
        ids = spot_ids((spots, 4 * rows), 0, dz)
        pick = ((ids == slot_rows[0]) | (ids == slot_rows[1])).astype(BF)
        outb[k] = dot(pick, stack[...]).astype(BF)
        if k == 0:
            pl.semaphore_wait(barrier, len(partners) + 2)
        for dx, dc in around:
            to = peer(dz, dx, dc)
            target = to[1] * cs + to[2]
            source = outb.at[k, pl.ds(pl.multiple_of(target * 16, 16), 16)]
            landing = inb.at[k, pl.ds(pl.multiple_of(me * 16, 16), 16)]
            if dz or dx or dc:
                remote(source, landing, dsend.at[k], drecv.at[k], to)
            else:
                landing[...] = source[...]

    def sized(buffer, k, dz):
        count = spots if dz else spots - 16
        return buffer.at[k, pl.ds(0, count)]

    halves = keep // 2

    def forward(k):
        wait_bytes(xg.at[k, 1], grecv.at[k, 0])
        remote(
            xg.at[k, 1, pl.ds(0, halves)],
            xg.at[k, 2, pl.ds(0, halves)],
            fsend.at[k, 0],
            frecv.at[k, 0],
            plus,
        )
        wait_bytes(xg.at[k, 3], grecv.at[k, 1])
        remote(
            xg.at[k, 3, pl.ds(halves, halves)],
            xg.at[k, 2, pl.ds(halves, halves)],
            fsend.at[k, 1],
            frecv.at[k, 1],
            minus,
        )

    for k, dz in enumerate(steps):
        if (spots if dz else spots - 16) > 0:
            wait_bytes(sized(inb, k, dz), drecv.at[k])
        tidy = dot(arrange, inb[k]).astype(BF)
        for n in range(4):
            xg[k, 0, :, n * cols : (n + 1) * cols] = tidy[n * keep : (n + 1) * keep]
        remote(xg.at[k, 0], xg.at[k, 1], gsend.at[k, 0], grecv.at[k, 0], plus)
        remote(xg.at[k, 0], xg.at[k, 3], gsend.at[k, 1], grecv.at[k, 1], minus)
        if k:
            forward(k - 1)
    forward(zs - 1)

    units = wg.shape[1]
    tiles = [(n, min(256, units - n)) for n in range(0, units, 256)]
    bundle = 2 if zs == 2 else zs // 2

    def back(k, dz):
        wait_bytes(ra.at[k, 0], arecv.at[k, 0])
        rs[k, 0] = (yb[k, 1, 0:halves].astype(F32) + ra[k, 0].astype(F32)).astype(BF)
        remote(rs.at[k, 0], rb.at[k, 0, pl.ds(0, halves)], ssend.at[k, 0], srecv.at[k, 0], minus)
        wait_bytes(ra.at[k, 1], arecv.at[k, 1])
        rs[k, 1] = (yb[k, 3, halves:keep].astype(F32) + ra[k, 1].astype(F32)).astype(BF)
        remote(
            rs.at[k, 1], rb.at[k, 1, pl.ds(halves, halves)], ssend.at[k, 1], srecv.at[k, 1], plus
        )

    def finish(k, dz):
        wait_bytes(rb.at[k, 0, pl.ds(halves, halves)], nrecv.at[k, 0])
        wait_bytes(rb.at[k, 1, pl.ds(0, halves)], nrecv.at[k, 1])
        wait_bytes(rb.at[k, 0, pl.ds(0, halves)], srecv.at[k, 0])
        wait_bytes(rb.at[k, 1, pl.ds(halves, halves)], srecv.at[k, 1])
        whole = yb[k, 0].astype(F32) + rb[k, 0].astype(F32) + rb[k, 1].astype(F32)
        whole = whole.astype(BF)
        laid = jnp.concatenate(
            [whole[:, n * cols : (n + 1) * cols] for n in range(4)], axis=0
        )
        backb[k] = dot(restore, laid).astype(BF)
        for dx, dc in around:
            to = peer((zs - dz) % zs, dx, dc)
            target = to[1] * cs + to[2]
            source = backb.at[k, pl.ds(pl.multiple_of(target * 16, 16), 16)]
            landing = retb.at[k, pl.ds(pl.multiple_of(me * 16, 16), 16)]
            if dz or dx or dc:
                remote(source, landing, bsend.at[k], brecv.at[k], to)
            else:
                landing[...] = source[...]

    for first in range(0, zs, bundle):
        chunk = range(first, first + bundle)
        for k in chunk:
            wait_bytes(xg.at[k, 2, pl.ds(0, halves)], frecv.at[k, 0])
            wait_bytes(xg.at[k, 2, pl.ds(halves, halves)], frecv.at[k, 1])
        if first == 0:
            loads[0].wait()
            loads[1].wait()
        big = bundle * ys * keep

        def gate_up(at, size):
            block = xg[first : first + bundle].reshape(big, model)
            gate = dot(block, wg[:, pl.ds(at, size)])
            up = dot(block, wu[:, pl.ds(at, size)])
            hid[:, pl.ds(at, size)] = (gate / (1.0 + jnp.exp(-gate)) * up).astype(BF)

        for at, size in tiles:
            gate_up(at, size)
        if first == 0:
            loads[2].wait()
        for at in range(0, model, 256):
            part = dot(hid[...], wd[:, at : at + 256]).astype(BF)
            yb[first : first + bundle, :, :, at : at + 256] = part.reshape(bundle, ys, keep, 256)
        for k in chunk:
            remote(yb.at[k, 2, pl.ds(0, halves)], ra.at[k, 0], asend.at[k, 0], arecv.at[k, 0], minus)
            remote(
                yb.at[k, 2, pl.ds(halves, halves)], ra.at[k, 1], asend.at[k, 1], arecv.at[k, 1], plus
            )
            remote(
                yb.at[k, 1, pl.ds(halves, halves)],
                rb.at[k, 0, pl.ds(halves, halves)],
                nsend.at[k, 0],
                nrecv.at[k, 0],
                minus,
            )
            remote(
                yb.at[k, 3, pl.ds(0, halves)],
                rb.at[k, 1, pl.ds(0, halves)],
                nsend.at[k, 1],
                nrecv.at[k, 1],
                plus,
            )
    for k, dz in enumerate(steps):
        back(k, dz)
        if k:
            finish(k - 1, steps[k - 1])
    finish(zs - 1, steps[-1])

    mix = jnp.zeros((4 * rows, cols), F32)
    for k, dz in enumerate(steps):
        if (spots if dz else spots - 16) > 0:
            wait_bytes(sized(retb, k, dz), brecv.at[k])
        ids = spot_ids((4 * rows, spots), 1, dz)
        share = jnp.where(ids == slot_cols[0], weight_cols[0], 0.0)
        share = share + jnp.where(ids == slot_cols[1], weight_cols[1], 0.0)
        high = share.astype(BF)
        low = (share - high.astype(F32)).astype(BF)
        mix = mix + dot(high, retb[k]) + dot(low, retb[k])
    mix = mix + stack[...].astype(F32)
    pieces = [mix[n * rows : (n + 1) * rows] for n in range(4)]
    center = sum(jnp.sum(piece, axis=1, keepdims=True) for piece in pieces) / model
    pieces = [piece - center for piece in pieces]
    spread = sum(jnp.sum(piece * piece, axis=1, keepdims=True) for piece in pieces) / model
    scale = lax.rsqrt(spread + eps_layer)
    for n in range(4):
        lanes = slice(n * cols, (n + 1) * cols)
        out_ref[:, lanes] = (
            pieces[n] * scale * gain_ref[1:2, lanes] + shift_ref[1:2, lanes]
        ).astype(BF)

    for k, dz in enumerate(steps):
        if (spots if dz else spots - 16) > 0:
            wait_bytes(sized(outb, k, dz), dsend.at[k])
            wait_bytes(sized(backb, k, dz), bsend.at[k])
        for n in range(2):
            wait_bytes(xg.at[k, 0], gsend.at[k, n])
            half = xg.at[k, 0, pl.ds(0, halves)]
            for sem in (fsend, asend, nsend, ssend):
                wait_bytes(half, sem.at[k, n])


def routed(sizes, *args):
    normed, wg = args[0], args[5]
    zs, xs, cs, ys = sizes
    rows, model = normed.shape
    units = wg.shape[2]
    group = xs * cs
    spots, keep, cols = group * 16, group * 4, model // 4
    bundle = 2 if zs == 2 else zs // 2
    dma = pltpu.SemaphoreType.DMA
    vmem = pl.BlockSpec(memory_space=pltpu.VMEM)
    hbm = pl.BlockSpec(memory_space=pl.ANY)
    return pl.pallas_call(
        functools.partial(experts_kernel, sizes),
        out_shape=jax.ShapeDtypeStruct((rows, model), BF),
        in_specs=[vmem] * 5 + [hbm] * 3,
        out_specs=vmem,
        scratch_shapes=[
            pltpu.VMEM((model, units), BF),
            pltpu.VMEM((model, units), BF),
            pltpu.VMEM((units, model), BF),
            pltpu.VMEM((4 * rows, cols), BF),
            pltpu.VMEM((zs, spots, cols), BF),
            pltpu.VMEM((zs, spots, cols), BF),
            pltpu.VMEM((zs, ys, keep, model), BF),
            pltpu.VMEM((bundle * ys * keep, units), BF),
            pltpu.VMEM((zs, ys, keep, model), BF),
            pltpu.VMEM((zs, 2, keep // 2, model), BF),
            pltpu.VMEM((zs, 2, keep // 2, model), BF),
            pltpu.VMEM((zs, 2, keep, model), BF),
            pltpu.VMEM((zs, spots, cols), BF),
            pltpu.VMEM((zs, spots, cols), BF),
            dma((3,)),
            dma((zs,)),
            dma((zs,)),
        ]
        + [dma((zs, 2))] * 10
        + [dma((zs,)), dma((zs,))],
        compiler_params=pltpu.CompilerParams(
            collective_id=1, has_side_effects=True, vmem_limit_bytes=60 * 1024 * 1024
        ),
        name="experts",
    )(*args)


def on_device(
    sizes,
    residual,
    queries,
    projected_keys,
    values,
    projected_output_gate,
    decay_gate_input,
    decay_gate_offset,
    decay_spikes,
    documents,
    attention_output_weight,
    layer_norm_gains,
    layer_norm_shifts,
    routes,
    chosen_expert_weights,
    expert_gate_weight,
    expert_up_weight,
    expert_down_weight,
):
    normed = attention(
        sizes,
        queries,
        projected_keys,
        values,
        projected_output_gate,
        decay_gate_input,
        decay_gate_offset.reshape(1, -1),
        decay_spikes,
        documents.reshape(1, -1),
        attention_output_weight,
        residual,
        layer_norm_gains,
        layer_norm_shifts,
    )
    return routed(
        sizes,
        normed,
        routes,
        chosen_expert_weights,
        layer_norm_gains,
        layer_norm_shifts,
        expert_gate_weight,
        expert_up_weight,
        expert_down_weight,
    )


def build(torus):
    sizes = tuple(torus.shape[a] for a in SP_TP)
    return jax.shard_map(
        functools.partial(on_device, sizes),
        mesh=torus,
        in_specs=(
            P(SP_TP, None),
            P(SP, "tp"),
            P(SP, "tp"),
            P(SP, "tp"),
            P(SP, "tp"),
            P(SP, "tp"),
            P("tp"),
            P(SP, "tp"),
            P(SP),
            P("tp", None),
            P(),
            P(),
            P(SP, None),
            P(SP, None),
            P(SP, None, "tp"),
            P(SP, None, "tp"),
            P(SP, "tp", None),
        ),
        out_specs=P(SP_TP, None),
        check_vma=False,
    )


def solution(mesh):
    return build(Mesh(mesh.devices.reshape(8, 4, 2, mesh.shape["tp"]), SP_TP))
```

```python
import functools

import jax
import jax.numpy as jnp
from jax import lax
from jax.experimental import pallas as pl
from jax.experimental.pallas import tpu as pltpu
from jax.sharding import Mesh
from jax.sharding import PartitionSpec as P

SP = ("sp_0", "sp_1", "sp_2")
SP_TP = ("sp_0", "sp_1", "sp_2", "tp")
MESH = pl.DeviceIdType.MESH
F32 = jnp.float32
BF = jnp.bfloat16
LAGS = (2, 3, 4, 6)
LEVELS = (1, 2, 4, 8, 16, 32, 64, 128)

eps_rms = 1e-06
eps_layer = 1e-05
decay_norm = 16.0


def dot(a, b):
    return jnp.dot(a, b, preferred_element_type=F32)


def dot_nt(a, b):
    return lax.dot_general(a, b, (((1,), (1,)), ((), ())), preferred_element_type=F32)


def dot_tn(a, b):
    return lax.dot_general(a, b, (((0,), (0,)), ((), ())), preferred_element_type=F32)


def iota(shape, dim):
    return lax.broadcasted_iota(jnp.int32, shape, dim)


def three_parts(a):
    high = a.astype(BF)
    rest = a - high.astype(F32)
    mid = rest.astype(BF)
    low = (rest - mid.astype(F32)).astype(BF)
    return high, mid, low


def offsets(count):
    order = [0]
    for d in range(1, count // 2 + 1):
        order.append(d)
        if count - d != d:
            order.append(count - d)
    return order


def plan(zs):
    direct = (0, 1, zs - 1) if zs >= 4 else (0,)
    steps = [2, 6, 3, 1, 5, 7, 4, 0] if zs == 8 else offsets(zs)[::-1]
    first = [k for k, dz in enumerate(steps) if dz not in direct]
    late = [k for k, dz in enumerate(steps) if dz in direct]
    return steps, first, late


def place(sizes):
    z, x, c, y = (lax.axis_index(a) for a in SP_TP)
    return z, x, c, y


def greet(partners):
    barrier = pltpu.get_barrier_semaphore()
    for partner in partners:
        pl.semaphore_signal(barrier, inc=1, device_id=partner, device_id_type=MESH)
    return barrier


def remote(src, dst, send_sem, recv_sem, device):
    copy = pltpu.make_async_remote_copy(
        src_ref=src,
        dst_ref=dst,
        send_sem=send_sem,
        recv_sem=recv_sem,
        device_id=device,
        device_id_type=MESH,
    )
    copy.start()
    return copy


def wait_bytes(ref, sem):
    pltpu.make_async_copy(ref, ref, sem).wait()


def level_reference(total, level):
    rows, width = total.shape
    if level >= 8:
        split = total.reshape(rows // (2 * level), 2 * level, width)
        return jnp.broadcast_to(split[:, level - 1 : level, :], split.shape).reshape(rows, width)
    split = total.reshape(rows // 8, 8, width)
    place_in = iota(split.shape, 1)
    row = split[:, level - 1 : level, :]
    for start in range(2 * level, 8, 2 * level):
        later = split[:, start + level - 1 : start + level, :]
        row = jnp.where(place_in >= start, later, row)
    return jnp.broadcast_to(row, split.shape).reshape(rows, width)


def message(state_t, decay_row, doc_row):
    high, mid, low = three_parts(decay_row)
    zeros = jnp.zeros((12, decay_row.shape[1]), F32)
    tail = jnp.concatenate(
        [high.astype(F32), mid.astype(F32), low.astype(F32), doc_row, zeros], axis=0
    )
    return jnp.concatenate([state_t.astype(BF), tail.astype(BF)], axis=0)


def opened(buffer, k, width):
    block = buffer[k].astype(F32)
    state = block[:width]
    decay = block[width : width + 1] + block[width + 1 : width + 2] + block[width + 2 : width + 3]
    return state, decay, block[width + 3 : width + 4]


NAMES = ("q", "k", "v", "g", "dgi", "off", "spk", "doc", "wo", "res", "gain", "shift")
NAMES = NAMES + ("routes", "weights")


def layer_kernel(sizes, *refs):
    hbm = dict(zip(NAMES, refs[: len(NAMES)]))
    wg_hbm, wu_hbm, wd_hbm, out_ref = refs[len(NAMES) : len(NAMES) + 4]
    refs = refs[len(NAMES) + 4 :]
    held = dict(zip(NAMES, refs[: len(NAMES)]))
    (
        isem,
        msg1,
        buf1,
        msg2,
        buf2,
        ql,
        kl,
        oacc,
        pb,
        far,
        near,
        summed,
        send1,
        recv1,
        send2,
        recv2,
        send3,
        recv3,
        wg,
        wu,
        wd,
        tok,
        mix,
        outb,
        inb,
        outq,
        inq,
        xg,
        hid,
        yb,
        ra,
        rs,
        rb,
        backb,
        retb,
        wsem,
        dsend,
        drecv,
        gsend,
        grecv,
        fsend,
        frecv,
        asend,
        arecv,
        nsend,
        nrecv,
        ssend,
        srecv,
        bsend,
        brecv,
        qsend,
        qrecv,
        tsend,
        trecv,
    ) = refs[len(NAMES) :]
    zs, xs, cs, ys = sizes
    z, x, c, y = place(sizes)
    group = xs * cs
    me = x * cs + c
    steps, routed, direct = plan(zs)
    around = [(dx, dc) for dx in range(xs) for dc in range(cs)]
    plus = (z, x, c, lax.rem(y + 1, ys))
    minus = (z, x, c, lax.rem(y + ys - 1, ys))

    def peer(dz, dx, dc):
        return (lax.rem(z + dz, zs), lax.rem(x + dx, xs), lax.rem(c + dc, cs), y)

    partners = [
        peer(dz, dx, dc) for dz in range(zs) for dx, dc in around if dz or dx or dc
    ]
    peers = [peer(0, dx, dc) for dx, dc in around if dx or dc]
    columns = [peer(dz, 0, 0) for dz in range(1, zs)]
    fills = {
        name: pltpu.make_async_copy(hbm[name], held[name], isem.at[n])
        for n, name in enumerate(NAMES)
    }
    for name in ("dgi", "off", "spk", "doc", "k", "v", "q"):
        fills[name].start()
    barrier = greet(partners + [plus, minus])
    for name in ("g", "wo", "routes", "weights", "res", "gain", "shift"):
        fills[name].start()
    loads = [
        pltpu.make_async_copy(src.at[0], dst, wsem.at[n])
        for n, (src, dst) in enumerate(((wg_hbm, wg), (wu_hbm, wu), (wd_hbm, wd)))
    ]
    for load in loads:
        load.start()
    for name in ("dgi", "off", "spk", "doc", "k", "v", "q"):
        fills[name].wait()

    length, hk = held["q"].shape
    hv = held["v"].shape[1]
    heads = held["spk"].shape[0]
    dk = hk // heads
    dv = hv // heads
    lane_head = iota((1, hk), 1) // dk
    vlane_head = iota((1, hv), 1) // dv

    pre = held["dgi"][...].astype(F32) + held["off"][...]
    rate = -(jnp.maximum(-pre, 0.0) + jnp.log1p(jnp.exp(-jnp.abs(pre)))) / decay_norm
    spikes = jnp.concatenate([p.astype(F32) for p in three_parts(held["spk"][...])], axis=0)
    spread_to = iota((3 * heads, hk), 0) % heads == iota((3 * heads, hk), 1) // dk
    rate = rate + dot_tn(spikes.astype(BF), spread_to.astype(BF))
    row_i = iota((length, length), 0)
    col_i = iota((length, length), 1)
    tri = (row_i >= col_i).astype(BF)
    high, mid, low = three_parts(rate)
    total = dot(tri, high) + dot(tri, mid) + dot(tri, low)
    last_total = total[length - 1 : length]

    doc_row = held["doc"][...].astype(F32)
    doc_col = jnp.sum(jnp.where(row_i == col_i, doc_row, 0.0), axis=1, keepdims=True)
    last_doc = doc_col[length - 1 : length]
    last_row = jnp.broadcast_to(last_doc, (1, hk))

    keys = held["k"][...].astype(F32)
    query = held["q"][...].astype(F32) * dk ** (-0.5)
    ends = keys * jnp.exp(jnp.minimum(last_total - total, 0.0))
    ends = jnp.where(doc_col == last_doc, ends, 0.0).astype(BF)
    cross = dot_tn(held["v"][...], ends)
    state_t = jnp.zeros((dv, hk), F32)
    for h in range(heads):
        state_t = state_t + jnp.where(lane_head == h, cross[h * dv : (h + 1) * dv], 0.0)
    first = message(state_t, last_total, last_row)
    msg1[...] = first
    buf1[me] = first
    pl.semaphore_wait(barrier, len(partners) + 2)
    for to in peers:
        remote(msg1, buf1.at[me], send1, recv1, to)

    ql[0] = query.astype(BF)
    kl[0] = keys.astype(BF)
    for n, level in enumerate(LEVELS):
        mark = level_reference(total, level)
        ql[n + 1] = (query * jnp.exp(jnp.minimum(total - mark, 0.0))).astype(BF)
        kl[n + 1] = (keys * jnp.exp(jnp.minimum(mark - total, 0.0))).astype(BF)
    entering = (query * jnp.exp(jnp.minimum(total, 0.0))).astype(BF)
    oacc[...] = jnp.zeros_like(oacc)
    visible = (row_i >= col_i) & (doc_col == doc_row)
    differ = row_i ^ col_i

    def head_work(h, carry):
        keep = lane_head == h
        scores = dot_nt(ql[0], jnp.where(keep, kl[0], jnp.zeros((), BF)))
        for n, level in enumerate(LEVELS):
            at_level = dot_nt(ql[n + 1], jnp.where(keep, kl[n + 1], jnp.zeros((), BF)))
            scores = jnp.where(differ >= level, at_level, scores)
        scores = jnp.where(visible, scores, 0.0).astype(BF)
        oacc[...] += dot(scores, jnp.where(vlane_head == h, held["v"][...], jnp.zeros((), BF)))
        return carry

    lax.fori_loop(0, heads // 2, head_work, 0)

    if group > 1:
        wait_bytes(buf1.at[pl.ds(0, group - 1)], recv1)
    parts = [opened(buf1, j, dv) for j in range(group)]
    group_doc = parts[group - 1][2]
    mine_doc = jnp.full((1, hk), -1.0, F32)
    for j in range(group - 1):
        mine_doc = jnp.where(me == j + 1, parts[j][2], mine_doc)
    group_state = jnp.zeros((dv, hk), F32)
    within = jnp.zeros((dv, hk), F32)
    group_decay = jnp.zeros((1, hk), F32)
    own_decay = jnp.zeros((1, hk), F32)
    for j in range(group - 1, -1, -1):
        state_j, decay_j, doc_j = parts[j]
        share = jnp.where(doc_j == group_doc, jnp.exp(jnp.minimum(group_decay, 0.0)), 0.0)
        group_state = group_state + share * state_j
        group_decay = group_decay + decay_j
        earlier = j < me
        share = jnp.where(doc_j == mine_doc, jnp.exp(jnp.minimum(own_decay, 0.0)), 0.0)
        within = within + jnp.where(earlier, share, 0.0) * state_j
        own_decay = own_decay + jnp.where(earlier, decay_j, 0.0)
    second = message(group_state, group_decay, group_doc)
    msg2[...] = second
    buf2[z] = second
    for to in columns:
        remote(msg2, buf2.at[z], send2, recv2, to)

    lax.fori_loop(heads // 2, heads, head_work, 0)

    fills["routes"].wait()
    fills["weights"].wait()
    rows = length // ys
    half = rows // 2
    model = held["wo"].shape[1]
    cols = model // 4
    spots = group * 16
    keep = group * 4
    halves = keep // 2
    experts = zs * group
    lanes = iota((rows, experts), 1).astype(F32)
    below = (iota((rows, rows), 0) > iota((rows, rows), 1)).astype(BF)
    quarter = (iota((4 * rows, 1), 0) // rows * 4).astype(F32)
    diagonal = iota((4 * rows, 4 * rows), 0) == iota((4 * rows, 4 * rows), 1)
    reach = iota((4 * rows, length), 1) - iota((4 * rows, length), 0) % rows

    def plane_col(name, j, plane):
        row = held[name][j : j + 1, :].astype(F32)
        mask = reach == lax.rem(y + plane, ys) * rows
        return jnp.sum(jnp.where(mask, row, 0.0), axis=1, keepdims=True)

    def plane_slots(plane):
        route_cols = [plane_col("routes", j, plane) for j in range(2)]
        marks = [(route_cols[j][0:rows] == lanes).astype(F32) for j in range(2)]
        before = dot(below, marks[0].astype(BF))
        pos0 = jnp.sum(before * marks[0], axis=1, keepdims=True)
        before = dot(below, marks[1].astype(BF)) + jnp.sum(marks[0], axis=0, keepdims=True)
        pos1 = jnp.sum(before * marks[1], axis=1, keepdims=True)
        slot_cols = []
        slot_rows = []
        for j, pos in ((0, pos0), (1, pos1)):
            one = route_cols[j] * 16 + jnp.concatenate([pos] * 4, axis=0) + quarter
            slot_cols.append(one.astype(jnp.int32))
            as_row = jnp.sum(jnp.where(diagonal, one, 0.0), axis=0, keepdims=True)
            slot_rows.append(as_row.astype(jnp.int32))
        return slot_cols, slot_rows

    planes = (0, ys - 1, 2, 1)
    slots = [plane_slots(planes[0])]
    slot_cols = slots[0][0]
    weight_cols = [plane_col("weights", j, 0) for j in range(2)]

    fills["g"].wait()
    fills["wo"].wait()
    gate = held["g"][...].astype(F32)
    gate = gate / (1.0 + jnp.exp(-gate))

    if zs > 1:
        wait_bytes(buf2.at[pl.ds(0, zs - 1)], recv2)
    parts = [opened(buf2, k, dv) for k in range(zs)]
    for k in range(zs - 1):
        mine_doc = jnp.where((me == 0) & (z == k + 1), parts[k][2], mine_doc)
    for k in range(zs - 1, -1, -1):
        state_k, decay_k, doc_k = parts[k]
        earlier = k < z
        share = jnp.where(doc_k == mine_doc, jnp.exp(jnp.minimum(own_decay, 0.0)), 0.0)
        within = within + jnp.where(earlier, share, 0.0) * state_k
        own_decay = own_decay + jnp.where(earlier, decay_k, 0.0)
    arriving = jnp.concatenate(
        [jnp.where(lane_head == h, within, 0.0).astype(BF) for h in range(heads)], axis=0
    )
    carried = dot_nt(entering, arriving)
    carried = jnp.where(doc_col == mine_doc[:, 0:1], carried, 0.0)
    recurrent = oacc[...] + carried
    same = (iota((hv, hv), 0) // dv == iota((hv, hv), 1) // dv).astype(BF)
    square = recurrent * recurrent
    square_high = square.astype(BF)
    square_low = (square - square_high.astype(F32)).astype(BF)
    mean = (dot(square_high, same) + dot(square_low, same)) / dv
    mixed = (recurrent * lax.rsqrt(mean + eps_rms) * gate).astype(BF)

    tile = model // 4
    for n in range(4):
        pb[:, n * tile : (n + 1) * tile] = dot(
            mixed, held["wo"][:, n * tile : (n + 1) * tile]
        ).astype(BF)

    def mine(offset, start):
        base = lax.rem(y + offset, ys) * rows + start
        return pb.at[pl.ds(pl.multiple_of(base, half), half)]

    remote(mine(2, 0), far.at[0], send3.at[0], recv3.at[0], minus)
    remote(mine(2, half), far.at[1], send3.at[1], recv3.at[1], plus)
    remote(mine(ys - 1, half), near.at[0, 1], send3.at[2], recv3.at[2], minus)
    remote(mine(1, 0), near.at[1, 0], send3.at[3], recv3.at[3], plus)
    slots = slots + [plane_slots(plane) for plane in planes[1:]]
    wait_bytes(far.at[0], recv3.at[0])
    summed[0] = (mine(ys - 1, 0)[...].astype(F32) + far[0].astype(F32)).astype(BF)
    remote(summed.at[0], near.at[0, 0], send3.at[4], recv3.at[4], minus)
    wait_bytes(far.at[1], recv3.at[1])
    summed[1] = (mine(1, half)[...].astype(F32) + far[1].astype(F32)).astype(BF)
    remote(summed.at[1], near.at[1, 1], send3.at[5], recv3.at[5], plus)
    for name in ("res", "gain", "shift"):
        fills[name].wait()
    gain = held["gain"][0:1, :]
    shift = held["shift"][0:1, :]
    wait_bytes(near.at[0, 1], recv3.at[2])
    wait_bytes(near.at[1, 0], recv3.at[3])
    wait_bytes(near.at[0, 0], recv3.at[4])
    wait_bytes(near.at[1, 1], recv3.at[5])
    for s in range(2):
        stream = held["res"][s * half : (s + 1) * half].astype(F32)
        stream = stream + mine(0, s * half)[...].astype(F32)
        stream = stream + near[0, s].astype(F32) + near[1, s].astype(F32)
        center = jnp.mean(stream, axis=-1, keepdims=True)
        moved = stream - center
        spread = jnp.mean(moved * moved, axis=-1, keepdims=True)
        normed = (moved * lax.rsqrt(spread + eps_layer) * gain + shift).astype(BF)
        for n in range(4):
            tok[0, n * rows + s * half : n * rows + (s + 1) * half] = normed[
                :, n * cols : (n + 1) * cols
            ]

    def spot_ids(shape, dim, dz):
        return iota(shape, dim) + lax.rem(z + dz, zs) * spots

    to_rows = iota((spots, spots), 0)
    from_rows = iota((spots, spots), 1)
    arranged = (to_rows % keep // 4) * 16 + (to_rows // keep) * 4 + to_rows % 4
    arrange = (from_rows == arranged).astype(BF)
    arranged = (from_rows % keep // 4) * 16 + (from_rows // keep) * 4 + from_rows % 4
    restore = (to_rows == arranged).astype(BF)

    def picked(p, dz):
        ids = spot_ids((spots, 4 * rows), 0, dz)
        pick = ((ids == slots[p][1][0]) | (ids == slots[p][1][1])).astype(BF)
        return dot(pick, tok[p]).astype(BF)

    def launch(k):
        dz = steps[k]
        if k in routed:
            out, into, send, recv, n = outb.at[k], inb.at[k], dsend, drecv, k
            out[...] = picked(0, dz)
        else:
            n = direct.index(k)
            out, into, send, recv = outq.at[n], inq.at[n], qsend, qrecv
            for p in range(ys):
                out[p] = picked(p, dz)
        for dx, dc in around:
            to = peer(dz, dx, dc)
            from_rows = pl.ds(pl.multiple_of((to[1] * cs + to[2]) * 16, 16), 16)
            to_rows = pl.ds(pl.multiple_of(me * 16, 16), 16)
            if k in routed:
                source, landing = out.at[from_rows], into.at[to_rows]
            else:
                source, landing = out.at[:, from_rows], into.at[:, to_rows]
            if dz or dx or dc:
                remote(source, landing, send.at[n], recv.at[n], to)
            else:
                landing[...] = source[...]

    remote(tok.at[0], tok.at[1], tsend.at[0], trecv.at[0], plus)
    remote(tok.at[0], tok.at[3], tsend.at[1], trecv.at[1], minus)
    for k in routed:
        launch(k)

    def sized(buffer, k, dz):
        count = spots if dz else spots - 16
        return buffer.at[k, pl.ds(0, count)]


    def forward(k):
        wait_bytes(xg.at[k, 1], grecv.at[k, 0])
        remote(
            xg.at[k, 1, pl.ds(0, halves)],
            xg.at[k, 2, pl.ds(0, halves)],
            fsend.at[k, 0],
            frecv.at[k, 0],
            plus,
        )
        wait_bytes(xg.at[k, 3], grecv.at[k, 1])
        remote(
            xg.at[k, 3, pl.ds(halves, halves)],
            xg.at[k, 2, pl.ds(halves, halves)],
            fsend.at[k, 1],
            frecv.at[k, 1],
            minus,
        )

    def tidied(block, k, p):
        flat = dot(arrange, block).astype(BF)
        for n in range(4):
            xg[k, p, :, n * cols : (n + 1) * cols] = flat[n * keep : (n + 1) * keep]

    def tidy(k):
        wait_bytes(inb.at[k], drecv.at[k])
        tidied(inb[k], k, 0)
        remote(xg.at[k, 0], xg.at[k, 1], gsend.at[k, 0], grecv.at[k, 0], plus)
        remote(xg.at[k, 0], xg.at[k, 3], gsend.at[k, 1], grecv.at[k, 1], minus)

    def sized_q(buffer, n):
        count = spots if steps[direct[n]] else spots - 16
        return buffer.at[n, :, pl.ds(0, count)]

    def arrived(k):
        if k in routed:
            wait_bytes(xg.at[k, 2, pl.ds(0, halves)], frecv.at[k, 0])
            wait_bytes(xg.at[k, 2, pl.ds(halves, halves)], frecv.at[k, 1])
            return
        n = direct.index(k)
        if steps[k] or group > 1:
            wait_bytes(sized_q(inq, n), qrecv.at[n])
        for p in range(ys):
            tidied(inq[n, p], k, p)

    units = wg.shape[1]
    tiles = [(n, min(256, units - n)) for n in range(0, units, 256)]

    def feed(k):
        arrived(k)
        if k == 0:
            loads[0].wait()
            loads[1].wait()
        for at, size in tiles:
            block = xg[k].reshape(ys * keep, model)
            gate = dot(block, wg[:, at : at + size])
            up = dot(block, wu[:, at : at + size])
            hid[:, at : at + size] = (gate / (1.0 + jnp.exp(-gate)) * up).astype(BF)
        if k == 0:
            loads[2].wait()
        for at in range(0, model, 256):
            part = dot(hid[...], wd[:, at : at + 256]).astype(BF)
            yb[k, :, :, at : at + 256] = part.reshape(ys, keep, 256)
        low, top = pl.ds(0, halves), pl.ds(halves, halves)
        remote(yb.at[k, 2, low], ra.at[k, 0], asend.at[k, 0], arecv.at[k, 0], minus)
        remote(yb.at[k, 2, top], ra.at[k, 1], asend.at[k, 1], arecv.at[k, 1], plus)
        remote(yb.at[k, 1, top], rb.at[k, 0, top], nsend.at[k, 0], nrecv.at[k, 0], minus)
        remote(yb.at[k, 3, low], rb.at[k, 1, low], nsend.at[k, 1], nrecv.at[k, 1], plus)

    def back(k, dz):
        wait_bytes(ra.at[k, 0], arecv.at[k, 0])
        rs[k, 0] = (yb[k, 1, 0:halves].astype(F32) + ra[k, 0].astype(F32)).astype(BF)
        remote(rs.at[k, 0], rb.at[k, 0, pl.ds(0, halves)], ssend.at[k, 0], srecv.at[k, 0], minus)
        wait_bytes(ra.at[k, 1], arecv.at[k, 1])
        rs[k, 1] = (yb[k, 3, halves:keep].astype(F32) + ra[k, 1].astype(F32)).astype(BF)
        remote(
            rs.at[k, 1], rb.at[k, 1, pl.ds(halves, halves)], ssend.at[k, 1], srecv.at[k, 1], plus
        )

    def finish(k, dz):
        wait_bytes(rb.at[k, 0, pl.ds(halves, halves)], nrecv.at[k, 0])
        wait_bytes(rb.at[k, 1, pl.ds(0, halves)], nrecv.at[k, 1])
        wait_bytes(rb.at[k, 0, pl.ds(0, halves)], srecv.at[k, 0])
        wait_bytes(rb.at[k, 1, pl.ds(halves, halves)], srecv.at[k, 1])
        whole = yb[k, 0].astype(F32) + rb[k, 0].astype(F32) + rb[k, 1].astype(F32)
        whole = whole.astype(BF)
        laid = jnp.concatenate(
            [whole[:, n * cols : (n + 1) * cols] for n in range(4)], axis=0
        )
        backb[k] = dot(restore, laid).astype(BF)
        for dx, dc in around:
            to = peer((zs - dz) % zs, dx, dc)
            target = to[1] * cs + to[2]
            source = backb.at[k, pl.ds(pl.multiple_of(target * 16, 16), 16)]
            landing = retb.at[k, pl.ds(pl.multiple_of(me * 16, 16), 16)]
            if dz or dx or dc:
                remote(source, landing, bsend.at[k], brecv.at[k], to)
            else:
                landing[...] = source[...]

    def gather_in(k, dz):
        if (spots if dz else spots - 16) > 0:
            wait_bytes(sized(retb, k, dz), brecv.at[k])
        ids = spot_ids((4 * rows, spots), 1, dz)
        share = jnp.where(ids == slot_cols[0], weight_cols[0], 0.0)
        share = share + jnp.where(ids == slot_cols[1], weight_cols[1], 0.0)
        high = share.astype(BF)
        low = (share - high.astype(F32)).astype(BF)
        mix[...] += dot(high, retb[k]) + dot(low, retb[k])

    low, top = pl.ds(0, 2 * rows), pl.ds(2 * rows, 2 * rows)
    wait_bytes(tok.at[1], trecv.at[0])
    remote(tok.at[1, low], tok.at[2, low], tsend.at[2], trecv.at[2], plus)
    wait_bytes(tok.at[3], trecv.at[1])
    remote(tok.at[3, top], tok.at[2, top], tsend.at[3], trecv.at[3], minus)
    mix[...] = tok[0].astype(F32)
    lag_m, lag_b, lag_e, lag_c = LAGS
    for t in range(zs + lag_c):
        if t < len(routed):
            tidy(routed[t])
        if t == 0:
            wait_bytes(tok.at[2, low], trecv.at[2])
            wait_bytes(tok.at[2, top], trecv.at[3])
            for k in direct:
                launch(k)
        if 1 <= t < len(routed) + 1:
            forward(routed[t - 1])
        if lag_m <= t < zs + lag_m:
            feed(t - lag_m)
        if lag_b <= t < zs + lag_b:
            back(t - lag_b, steps[t - lag_b])
        if lag_e <= t < zs + lag_e:
            finish(t - lag_e, steps[t - lag_e])
        if lag_c <= t < zs + lag_c:
            gather_in(t - lag_c, steps[t - lag_c])

    pieces = [mix[n * rows : (n + 1) * rows] for n in range(4)]
    center = sum(jnp.sum(piece, axis=1, keepdims=True) for piece in pieces) / model
    pieces = [piece - center for piece in pieces]
    spread = sum(jnp.sum(piece * piece, axis=1, keepdims=True) for piece in pieces) / model
    scale = lax.rsqrt(spread + eps_layer)
    for n in range(4):
        at = slice(n * cols, (n + 1) * cols)
        out_ref[:, at] = (
            pieces[n] * scale * held["gain"][1:2, at] + held["shift"][1:2, at]
        ).astype(BF)

    if group > 1:
        wait_bytes(buf1.at[pl.ds(0, group - 1)], send1)
    if zs > 1:
        wait_bytes(buf2.at[pl.ds(0, zs - 1)], send2)
    for n in range(6):
        wait_bytes(far.at[0], send3.at[n])
    for n in range(2):
        wait_bytes(tok.at[0], tsend.at[n])
        wait_bytes(tok.at[2, low], tsend.at[n + 2])
    for k, dz in enumerate(steps):
        part = xg.at[k, 0, pl.ds(0, halves)]
        if k in routed:
            wait_bytes(outb.at[k], dsend.at[k])
            for n in range(2):
                wait_bytes(xg.at[k, 0], gsend.at[k, n])
                wait_bytes(part, fsend.at[k, n])
        elif dz or group > 1:
            wait_bytes(sized_q(outq, direct.index(k)), qsend.at[direct.index(k)])
        if dz or group > 1:
            wait_bytes(sized(backb, k, dz), bsend.at[k])
        for n in range(2):
            for sem in (asend, nsend, ssend):
                wait_bytes(part, sem.at[k, n])


def layer(sizes, *args):
    named = dict(zip(NAMES, args))
    wg = args[-3]
    zs, xs, cs, ys = sizes
    length, hk = named["q"].shape
    hv = named["v"].shape[1]
    dv = hv // named["spk"].shape[0]
    rows, model = named["res"].shape
    units = wg.shape[2]
    group = xs * cs
    spots, keep, cols = group * 16, group * 4, model // 4
    dma = pltpu.SemaphoreType.DMA
    hbm = pl.BlockSpec(memory_space=pl.ANY)
    half = rows // 2
    wide = len(plan(zs)[2])
    return pl.pallas_call(
        functools.partial(layer_kernel, sizes),
        out_shape=jax.ShapeDtypeStruct((rows, model), BF),
        in_specs=[hbm] * len(args),
        out_specs=pl.BlockSpec(memory_space=pltpu.VMEM),
        scratch_shapes=[pltpu.VMEM(named[name].shape, named[name].dtype) for name in NAMES]
        + [
            dma((len(NAMES),)),
            pltpu.VMEM((dv + 16, hk), BF),
            pltpu.VMEM((group, dv + 16, hk), BF),
            pltpu.VMEM((dv + 16, hk), BF),
            pltpu.VMEM((zs, dv + 16, hk), BF),
            pltpu.VMEM((len(LEVELS) + 1, length, hk), BF),
            pltpu.VMEM((len(LEVELS) + 1, length, hk), BF),
            pltpu.VMEM((length, hv), F32),
            pltpu.VMEM((length, model), BF),
            pltpu.VMEM((2, half, model), BF),
            pltpu.VMEM((2, 2, half, model), BF),
            pltpu.VMEM((2, half, model), BF),
            dma,
            dma,
            dma,
            dma,
            dma((6,)),
            dma((6,)),
            pltpu.VMEM((model, units), BF),
            pltpu.VMEM((model, units), BF),
            pltpu.VMEM((units, model), BF),
            pltpu.VMEM((4, 4 * rows, cols), BF),
            pltpu.VMEM((4 * rows, cols), F32),
            pltpu.VMEM((zs, spots, cols), BF),
            pltpu.VMEM((zs, spots, cols), BF),
            pltpu.VMEM((wide, 4, spots, cols), BF),
            pltpu.VMEM((wide, 4, spots, cols), BF),
            pltpu.VMEM((zs, ys, keep, model), BF),
            pltpu.VMEM((ys * keep, units), BF),
            pltpu.VMEM((zs, ys, keep, model), BF),
            pltpu.VMEM((zs, 2, keep // 2, model), BF),
            pltpu.VMEM((zs, 2, keep // 2, model), BF),
            pltpu.VMEM((zs, 2, keep, model), BF),
            pltpu.VMEM((zs, spots, cols), BF),
            pltpu.VMEM((zs, spots, cols), BF),
            dma((3,)),
            dma((zs,)),
            dma((zs,)),
        ]
        + [dma((zs, 2))] * 10
        + [dma((zs,)), dma((zs,)), dma((wide,)), dma((wide,)), dma((4,)), dma((4,))],
        compiler_params=pltpu.CompilerParams(
            collective_id=0, has_side_effects=True, vmem_limit_bytes=44 * 1024 * 1024
        ),
        name="layer",
    )(*[pltpu.with_memory_space_constraint(a, pltpu.HBM) for a in args])


def on_device(
    sizes,
    residual,
    queries,
    projected_keys,
    values,
    projected_output_gate,
    decay_gate_input,
    decay_gate_offset,
    decay_spikes,
    documents,
    attention_output_weight,
    layer_norm_gains,
    layer_norm_shifts,
    routes,
    chosen_expert_weights,
    expert_gate_weight,
    expert_up_weight,
    expert_down_weight,
):
    return layer(
        sizes,
        queries,
        projected_keys,
        values,
        projected_output_gate,
        decay_gate_input,
        decay_gate_offset.reshape(1, -1),
        decay_spikes.T,
        documents.reshape(1, -1),
        attention_output_weight,
        residual,
        layer_norm_gains,
        layer_norm_shifts,
        routes.T,
        chosen_expert_weights.T,
        expert_gate_weight,
        expert_up_weight,
        expert_down_weight,
    )


def build(torus):
    sizes = tuple(torus.shape[a] for a in SP_TP)
    return jax.shard_map(
        functools.partial(on_device, sizes),
        mesh=torus,
        in_specs=(
            P(SP_TP, None),
            P(SP, "tp"),
            P(SP, "tp"),
            P(SP, "tp"),
            P(SP, "tp"),
            P(SP, "tp"),
            P("tp"),
            P(SP, "tp"),
            P(SP),
            P("tp", None),
            P(),
            P(),
            P(SP, None),
            P(SP, None),
            P(SP, None, "tp"),
            P(SP, None, "tp"),
            P(SP, "tp", None),
        ),
        out_specs=P(SP_TP, None),
        check_vma=False,
    )


def solution(mesh):
    return build(Mesh(mesh.devices.reshape(8, 4, 2, mesh.shape["tp"]), SP_TP))
```

```python
import functools

import jax
import jax.numpy as jnp
from jax import lax
from jax.experimental import pallas as pl
from jax.experimental.pallas import tpu as pltpu
from jax.sharding import Mesh
from jax.sharding import PartitionSpec as P

SP = ("sp_0", "sp_1", "sp_2")
SP_TP = ("sp_0", "sp_1", "sp_2", "tp")
MESH = pl.DeviceIdType.MESH
F32 = jnp.float32
BF = jnp.bfloat16
LAGS = (2, 3, 4, 8)
LEVELS = (1, 2, 4, 8, 16, 32, 64, 128)

eps_rms = 1e-06
eps_layer = 1e-05
decay_norm = 16.0


def dot(a, b):
    return jnp.dot(a, b, preferred_element_type=F32)


def dot_nt(a, b):
    return lax.dot_general(a, b, (((1,), (1,)), ((), ())), preferred_element_type=F32)


def dot_tn(a, b):
    return lax.dot_general(a, b, (((0,), (0,)), ((), ())), preferred_element_type=F32)


def iota(shape, dim):
    return lax.broadcasted_iota(jnp.int32, shape, dim)


def three_parts(a):
    high = a.astype(BF)
    rest = a - high.astype(F32)
    mid = rest.astype(BF)
    low = (rest - mid.astype(F32)).astype(BF)
    return high, mid, low


def offsets(count):
    order = [0]
    for d in range(1, count // 2 + 1):
        order.append(d)
        if count - d != d:
            order.append(count - d)
    return order


def plan(zs):
    direct = (0, 1, zs - 1) if zs >= 4 else (0,)
    steps = [2, 6, 3, 5, 1, 4, 7, 0] if zs == 8 else offsets(zs)[::-1]
    first = [k for k, dz in enumerate(steps) if dz not in direct]
    late = [k for k, dz in enumerate(steps) if dz in direct]
    return steps, first, late


def place(sizes):
    z, x, c, y = (lax.axis_index(a) for a in SP_TP)
    return z, x, c, y


def greet(partners):
    barrier = pltpu.get_barrier_semaphore()
    for partner in partners:
        pl.semaphore_signal(barrier, inc=1, device_id=partner, device_id_type=MESH)
    return barrier


def remote(src, dst, send_sem, recv_sem, device):
    copy = pltpu.make_async_remote_copy(
        src_ref=src,
        dst_ref=dst,
        send_sem=send_sem,
        recv_sem=recv_sem,
        device_id=device,
        device_id_type=MESH,
    )
    copy.start()
    return copy


def wait_bytes(ref, sem):
    pltpu.make_async_copy(ref, ref, sem).wait()


def level_reference(total, level):
    rows, width = total.shape
    if level >= 8:
        split = total.reshape(rows // (2 * level), 2 * level, width)
        return jnp.broadcast_to(split[:, level - 1 : level, :], split.shape).reshape(rows, width)
    split = total.reshape(rows // 8, 8, width)
    place_in = iota(split.shape, 1)
    row = split[:, level - 1 : level, :]
    for start in range(2 * level, 8, 2 * level):
        later = split[:, start + level - 1 : start + level, :]
        row = jnp.where(place_in >= start, later, row)
    return jnp.broadcast_to(row, split.shape).reshape(rows, width)


def message(state_t, decay_row, doc_row):
    high, mid, low = three_parts(decay_row)
    zeros = jnp.zeros((12, decay_row.shape[1]), F32)
    tail = jnp.concatenate(
        [high.astype(F32), mid.astype(F32), low.astype(F32), doc_row, zeros], axis=0
    )
    return jnp.concatenate([state_t.astype(BF), tail.astype(BF)], axis=0)


def opened(buffer, k, width):
    block = buffer[k].astype(F32)
    state = block[:width]
    decay = block[width : width + 1] + block[width + 1 : width + 2] + block[width + 2 : width + 3]
    return state, decay, block[width + 3 : width + 4]


NAMES = ("q", "k", "v", "g", "dgi", "off", "spk", "doc", "wo", "res", "gain", "shift")
NAMES = NAMES + ("routes", "weights")


def layer_kernel(sizes, *refs):
    hbm = dict(zip(NAMES, refs[: len(NAMES)]))
    wg_hbm, wu_hbm, wd_hbm, out_ref = refs[len(NAMES) : len(NAMES) + 4]
    refs = refs[len(NAMES) + 4 :]
    held = dict(zip(NAMES, refs[: len(NAMES)]))
    (
        isem,
        msg1,
        buf1,
        msg2,
        buf2,
        ql,
        kl,
        oacc,
        pb,
        far,
        near,
        summed,
        send1,
        recv1,
        send2,
        recv2,
        send3,
        recv3,
        wg,
        wu,
        wd,
        tok,
        mix,
        outb,
        inb,
        outq,
        inq,
        xg,
        hid,
        yb,
        ra,
        rs,
        rb,
        backb,
        retb,
        wsem,
        dsend,
        drecv,
        gsend,
        grecv,
        fsend,
        frecv,
        asend,
        arecv,
        nsend,
        nrecv,
        ssend,
        srecv,
        bsend,
        brecv,
        qsend,
        qrecv,
        tsend,
        trecv,
    ) = refs[len(NAMES) :]
    zs, xs, cs, ys = sizes
    z, x, c, y = place(sizes)
    group = xs * cs
    me = x * cs + c
    steps, routed, direct = plan(zs)
    around = [(dx, dc) for dx in range(xs) for dc in range(cs)]
    plus = (z, x, c, lax.rem(y + 1, ys))
    minus = (z, x, c, lax.rem(y + ys - 1, ys))

    def peer(dz, dx, dc):
        return (lax.rem(z + dz, zs), lax.rem(x + dx, xs), lax.rem(c + dc, cs), y)

    partners = [
        peer(dz, dx, dc) for dz in range(zs) for dx, dc in around if dz or dx or dc
    ]
    peers = [peer(0, dx, dc) for dx, dc in around if dx or dc]
    columns = [peer(dz, 0, 0) for dz in range(1, zs)]
    fills = {
        name: pltpu.make_async_copy(hbm[name], held[name], isem.at[n])
        for n, name in enumerate(NAMES)
    }
    for name in ("dgi", "off", "spk", "doc", "k", "v", "q"):
        fills[name].start()
    barrier = greet(partners + [plus, minus])
    for name in ("g", "wo", "routes", "weights", "res", "gain", "shift"):
        fills[name].start()
    loads = [
        pltpu.make_async_copy(src.at[0], dst, wsem.at[n])
        for n, (src, dst) in enumerate(((wg_hbm, wg), (wu_hbm, wu), (wd_hbm, wd)))
    ]
    for load in loads:
        load.start()
    for name in ("dgi", "off", "spk", "doc", "k", "v", "q"):
        fills[name].wait()

    length, hk = held["q"].shape
    hv = held["v"].shape[1]
    heads = held["spk"].shape[0]
    dk = hk // heads
    dv = hv // heads
    lane_head = iota((1, hk), 1) // dk
    vlane_head = iota((1, hv), 1) // dv

    pre = held["dgi"][...].astype(F32) + held["off"][...]
    rate = -(jnp.maximum(-pre, 0.0) + jnp.log1p(jnp.exp(-jnp.abs(pre)))) / decay_norm
    spikes = jnp.concatenate([p.astype(F32) for p in three_parts(held["spk"][...])], axis=0)
    spread_to = iota((3 * heads, hk), 0) % heads == iota((3 * heads, hk), 1) // dk
    rate = rate + dot_tn(spikes.astype(BF), spread_to.astype(BF))
    row_i = iota((length, length), 0)
    col_i = iota((length, length), 1)
    tri = (row_i >= col_i).astype(BF)
    high, mid, low = three_parts(rate)
    total = dot(tri, high) + dot(tri, mid) + dot(tri, low)
    last_total = total[length - 1 : length]

    doc_row = held["doc"][...].astype(F32)
    doc_col = jnp.sum(jnp.where(row_i == col_i, doc_row, 0.0), axis=1, keepdims=True)
    last_doc = doc_col[length - 1 : length]
    last_row = jnp.broadcast_to(last_doc, (1, hk))

    keys = held["k"][...].astype(F32)
    query = held["q"][...].astype(F32) * dk ** (-0.5)
    ends = keys * jnp.exp(jnp.minimum(last_total - total, 0.0))
    ends = jnp.where(doc_col == last_doc, ends, 0.0).astype(BF)
    cross = dot_tn(held["v"][...], ends)
    state_t = jnp.zeros((dv, hk), F32)
    for h in range(heads):
        state_t = state_t + jnp.where(lane_head == h, cross[h * dv : (h + 1) * dv], 0.0)
    first = message(state_t, last_total, last_row)
    msg1[...] = first
    buf1[me] = first
    pl.semaphore_wait(barrier, len(partners) + 2)
    for to in peers:
        remote(msg1, buf1.at[me], send1, recv1, to)

    ql[0] = query.astype(BF)
    kl[0] = keys.astype(BF)
    for n, level in enumerate(LEVELS):
        mark = level_reference(total, level)
        ql[n + 1] = (query * jnp.exp(jnp.minimum(total - mark, 0.0))).astype(BF)
        kl[n + 1] = (keys * jnp.exp(jnp.minimum(mark - total, 0.0))).astype(BF)
    entering = (query * jnp.exp(jnp.minimum(total, 0.0))).astype(BF)
    oacc[...] = jnp.zeros_like(oacc)
    visible = (row_i >= col_i) & (doc_col == doc_row)
    differ = row_i ^ col_i

    def head_work(h, carry):
        keep = lane_head == h
        scores = dot_nt(ql[0], jnp.where(keep, kl[0], jnp.zeros((), BF)))
        for n, level in enumerate(LEVELS):
            at_level = dot_nt(ql[n + 1], jnp.where(keep, kl[n + 1], jnp.zeros((), BF)))
            scores = jnp.where(differ >= level, at_level, scores)
        scores = jnp.where(visible, scores, 0.0).astype(BF)
        oacc[...] += dot(scores, jnp.where(vlane_head == h, held["v"][...], jnp.zeros((), BF)))
        return carry

    lax.fori_loop(0, heads // 2, head_work, 0)

    if group > 1:
        wait_bytes(buf1.at[pl.ds(0, group - 1)], recv1)
    parts = [opened(buf1, j, dv) for j in range(group)]
    group_doc = parts[group - 1][2]
    mine_doc = jnp.full((1, hk), -1.0, F32)
    for j in range(group - 1):
        mine_doc = jnp.where(me == j + 1, parts[j][2], mine_doc)
    group_state = jnp.zeros((dv, hk), F32)
    within = jnp.zeros((dv, hk), F32)
    group_decay = jnp.zeros((1, hk), F32)
    own_decay = jnp.zeros((1, hk), F32)
    for j in range(group - 1, -1, -1):
        state_j, decay_j, doc_j = parts[j]
        share = jnp.where(doc_j == group_doc, jnp.exp(jnp.minimum(group_decay, 0.0)), 0.0)
        group_state = group_state + share * state_j
        group_decay = group_decay + decay_j
        earlier = j < me
        share = jnp.where(doc_j == mine_doc, jnp.exp(jnp.minimum(own_decay, 0.0)), 0.0)
        within = within + jnp.where(earlier, share, 0.0) * state_j
        own_decay = own_decay + jnp.where(earlier, decay_j, 0.0)
    second = message(group_state, group_decay, group_doc)
    msg2[...] = second
    buf2[z] = second
    for to in columns:
        remote(msg2, buf2.at[z], send2, recv2, to)

    lax.fori_loop(heads // 2, heads, head_work, 0)

    fills["routes"].wait()
    fills["weights"].wait()
    rows = length // ys
    half = rows // 2
    model = held["wo"].shape[1]
    cols = model // 4
    spots = group * 16
    keep = group * 4
    halves = keep // 2
    experts = zs * group
    lanes = iota((rows, experts), 1).astype(F32)
    below = (iota((rows, rows), 0) > iota((rows, rows), 1)).astype(BF)
    quarter = (iota((4 * rows, 1), 0) // rows * 4).astype(F32)
    diagonal = iota((4 * rows, 4 * rows), 0) == iota((4 * rows, 4 * rows), 1)
    reach = iota((4 * rows, length), 1) - iota((4 * rows, length), 0) % rows

    def plane_col(name, j, plane):
        row = held[name][j : j + 1, :].astype(F32)
        mask = reach == lax.rem(y + plane, ys) * rows
        return jnp.sum(jnp.where(mask, row, 0.0), axis=1, keepdims=True)

    def plane_slots(plane):
        route_cols = [plane_col("routes", j, plane) for j in range(2)]
        marks = [(route_cols[j][0:rows] == lanes).astype(F32) for j in range(2)]
        before = dot(below, marks[0].astype(BF))
        pos0 = jnp.sum(before * marks[0], axis=1, keepdims=True)
        before = dot(below, marks[1].astype(BF)) + jnp.sum(marks[0], axis=0, keepdims=True)
        pos1 = jnp.sum(before * marks[1], axis=1, keepdims=True)
        slot_cols = []
        slot_rows = []
        for j, pos in ((0, pos0), (1, pos1)):
            one = route_cols[j] * 16 + jnp.concatenate([pos] * 4, axis=0) + quarter
            slot_cols.append(one.astype(jnp.int32))
            as_row = jnp.sum(jnp.where(diagonal, one, 0.0), axis=0, keepdims=True)
            slot_rows.append(as_row.astype(jnp.int32))
        return slot_cols, slot_rows

    planes = (0, ys - 1, 2, 1)
    slots = [plane_slots(planes[0])]
    slot_cols = slots[0][0]
    weight_cols = [plane_col("weights", j, 0) for j in range(2)]

    fills["g"].wait()
    fills["wo"].wait()
    gate = held["g"][...].astype(F32)
    gate = gate / (1.0 + jnp.exp(-gate))

    if zs > 1:
        wait_bytes(buf2.at[pl.ds(0, zs - 1)], recv2)
    parts = [opened(buf2, k, dv) for k in range(zs)]
    for k in range(zs - 1):
        mine_doc = jnp.where((me == 0) & (z == k + 1), parts[k][2], mine_doc)
    for k in range(zs - 1, -1, -1):
        state_k, decay_k, doc_k = parts[k]
        earlier = k < z
        share = jnp.where(doc_k == mine_doc, jnp.exp(jnp.minimum(own_decay, 0.0)), 0.0)
        within = within + jnp.where(earlier, share, 0.0) * state_k
        own_decay = own_decay + jnp.where(earlier, decay_k, 0.0)
    arriving = jnp.concatenate(
        [jnp.where(lane_head == h, within, 0.0).astype(BF) for h in range(heads)], axis=0
    )
    carried = dot_nt(entering, arriving)
    carried = jnp.where(doc_col == mine_doc[:, 0:1], carried, 0.0)
    recurrent = oacc[...] + carried
    same = (iota((hv, hv), 0) // dv == iota((hv, hv), 1) // dv).astype(BF)
    square = recurrent * recurrent
    square_high = square.astype(BF)
    square_low = (square - square_high.astype(F32)).astype(BF)
    mean = (dot(square_high, same) + dot(square_low, same)) / dv
    mixed = (recurrent * lax.rsqrt(mean + eps_rms) * gate).astype(BF)

    tile = model // 4
    for n in range(4):
        pb[:, n * tile : (n + 1) * tile] = dot(
            mixed, held["wo"][:, n * tile : (n + 1) * tile]
        ).astype(BF)

    def mine(offset, start):
        base = lax.rem(y + offset, ys) * rows + start
        return pb.at[pl.ds(pl.multiple_of(base, half), half)]

    remote(mine(2, 0), far.at[0], send3.at[0], recv3.at[0], minus)
    remote(mine(2, half), far.at[1], send3.at[1], recv3.at[1], plus)
    remote(mine(ys - 1, half), near.at[0, 1], send3.at[2], recv3.at[2], minus)
    remote(mine(1, 0), near.at[1, 0], send3.at[3], recv3.at[3], plus)
    slots = slots + [plane_slots(plane) for plane in planes[1:]]
    wait_bytes(far.at[0], recv3.at[0])
    summed[0] = (mine(ys - 1, 0)[...].astype(F32) + far[0].astype(F32)).astype(BF)
    remote(summed.at[0], near.at[0, 0], send3.at[4], recv3.at[4], minus)
    wait_bytes(far.at[1], recv3.at[1])
    summed[1] = (mine(1, half)[...].astype(F32) + far[1].astype(F32)).astype(BF)
    remote(summed.at[1], near.at[1, 1], send3.at[5], recv3.at[5], plus)
    for name in ("res", "gain", "shift"):
        fills[name].wait()
    gain = held["gain"][0:1, :]
    shift = held["shift"][0:1, :]
    wait_bytes(near.at[0, 1], recv3.at[2])
    wait_bytes(near.at[1, 0], recv3.at[3])
    wait_bytes(near.at[0, 0], recv3.at[4])
    wait_bytes(near.at[1, 1], recv3.at[5])
    for s in range(2):
        stream = held["res"][s * half : (s + 1) * half].astype(F32)
        stream = stream + mine(0, s * half)[...].astype(F32)
        stream = stream + near[0, s].astype(F32) + near[1, s].astype(F32)
        center = jnp.mean(stream, axis=-1, keepdims=True)
        moved = stream - center
        spread = jnp.mean(moved * moved, axis=-1, keepdims=True)
        normed = (moved * lax.rsqrt(spread + eps_layer) * gain + shift).astype(BF)
        for n in range(4):
            tok[0, n * rows + s * half : n * rows + (s + 1) * half] = normed[
                :, n * cols : (n + 1) * cols
            ]

    def spot_ids(shape, dim, dz):
        return iota(shape, dim) + lax.rem(z + dz, zs) * spots

    to_rows = iota((spots, spots), 0)
    from_rows = iota((spots, spots), 1)
    arranged = (to_rows % keep // 4) * 16 + (to_rows // keep) * 4 + to_rows % 4
    arrange = (from_rows == arranged).astype(BF)
    arranged = (from_rows % keep // 4) * 16 + (from_rows // keep) * 4 + from_rows % 4
    restore = (to_rows == arranged).astype(BF)

    def picked(p, dz):
        ids = spot_ids((spots, 4 * rows), 0, dz)
        pick = ((ids == slots[p][1][0]) | (ids == slots[p][1][1])).astype(BF)
        return dot(pick, tok[p]).astype(BF)

    def launch(k):
        dz = steps[k]
        if k in routed:
            out, into, send, recv, n = outb.at[k], inb.at[k], dsend, drecv, k
            out[...] = picked(0, dz)
        else:
            n = direct.index(k)
            out, into, send, recv = outq.at[n], inq.at[n], qsend, qrecv
            for p in range(ys):
                out[p] = picked(p, dz)
        for dx, dc in around:
            to = peer(dz, dx, dc)
            from_rows = pl.ds(pl.multiple_of((to[1] * cs + to[2]) * 16, 16), 16)
            to_rows = pl.ds(pl.multiple_of(me * 16, 16), 16)
            if k in routed:
                source, landing = out.at[from_rows], into.at[to_rows]
            else:
                source, landing = out.at[:, from_rows], into.at[:, to_rows]
            if dz or dx or dc:
                remote(source, landing, send.at[n], recv.at[n], to)
            else:
                landing[...] = source[...]

    remote(tok.at[0], tok.at[1], tsend.at[0], trecv.at[0], plus)
    remote(tok.at[0], tok.at[3], tsend.at[1], trecv.at[1], minus)
    for k in routed:
        launch(k)

    def sized(buffer, k, dz):
        count = spots if dz else spots - 16
        return buffer.at[k, pl.ds(0, count)]


    def forward(k):
        wait_bytes(xg.at[k, 1], grecv.at[k, 0])
        remote(
            xg.at[k, 1, pl.ds(0, halves)],
            xg.at[k, 2, pl.ds(0, halves)],
            fsend.at[k, 0],
            frecv.at[k, 0],
            plus,
        )
        wait_bytes(xg.at[k, 3], grecv.at[k, 1])
        remote(
            xg.at[k, 3, pl.ds(halves, halves)],
            xg.at[k, 2, pl.ds(halves, halves)],
            fsend.at[k, 1],
            frecv.at[k, 1],
            minus,
        )

    def tidied(block, k, p):
        flat = dot(arrange, block).astype(BF)
        for n in range(4):
            xg[k, p, :, n * cols : (n + 1) * cols] = flat[n * keep : (n + 1) * keep]

    def tidy(k):
        wait_bytes(inb.at[k], drecv.at[k])
        tidied(inb[k], k, 0)
        remote(xg.at[k, 0], xg.at[k, 1], gsend.at[k, 0], grecv.at[k, 0], plus)
        remote(xg.at[k, 0], xg.at[k, 3], gsend.at[k, 1], grecv.at[k, 1], minus)

    def sized_q(buffer, n):
        count = spots if steps[direct[n]] else spots - 16
        return buffer.at[n, :, pl.ds(0, count)]

    def arrived(k):
        if k in routed:
            wait_bytes(xg.at[k, 2, pl.ds(0, halves)], frecv.at[k, 0])
            wait_bytes(xg.at[k, 2, pl.ds(halves, halves)], frecv.at[k, 1])
            return
        n = direct.index(k)
        if steps[k] or group > 1:
            wait_bytes(sized_q(inq, n), qrecv.at[n])
        for p in range(ys):
            tidied(inq[n, p], k, p)

    units = wg.shape[1]
    tiles = [(n, min(256, units - n)) for n in range(0, units, 256)]

    def feed(k):
        arrived(k)
        if k == 0:
            loads[0].wait()
            loads[1].wait()
        for at, size in tiles:
            block = xg[k].reshape(ys * keep, model)
            gate = dot(block, wg[:, at : at + size])
            up = dot(block, wu[:, at : at + size])
            hid[:, at : at + size] = (gate / (1.0 + jnp.exp(-gate)) * up).astype(BF)
        if k == 0:
            loads[2].wait()
        for at in range(0, model, 256):
            part = dot(hid[...], wd[:, at : at + 256]).astype(BF)
            yb[k, :, :, at : at + 256] = part.reshape(ys, keep, 256)
        low, top = pl.ds(0, halves), pl.ds(halves, halves)
        remote(yb.at[k, 2, low], ra.at[k, 0], asend.at[k, 0], arecv.at[k, 0], minus)
        remote(yb.at[k, 2, top], ra.at[k, 1], asend.at[k, 1], arecv.at[k, 1], plus)
        remote(yb.at[k, 1, top], rb.at[k, 0, top], nsend.at[k, 0], nrecv.at[k, 0], minus)
        remote(yb.at[k, 3, low], rb.at[k, 1, low], nsend.at[k, 1], nrecv.at[k, 1], plus)

    def back(k, dz):
        wait_bytes(ra.at[k, 0], arecv.at[k, 0])
        rs[k, 0] = (yb[k, 1, 0:halves].astype(F32) + ra[k, 0].astype(F32)).astype(BF)
        remote(rs.at[k, 0], rb.at[k, 0, pl.ds(0, halves)], ssend.at[k, 0], srecv.at[k, 0], minus)
        wait_bytes(ra.at[k, 1], arecv.at[k, 1])
        rs[k, 1] = (yb[k, 3, halves:keep].astype(F32) + ra[k, 1].astype(F32)).astype(BF)
        remote(
            rs.at[k, 1], rb.at[k, 1, pl.ds(halves, halves)], ssend.at[k, 1], srecv.at[k, 1], plus
        )

    def finish(k, dz):
        wait_bytes(rb.at[k, 0, pl.ds(halves, halves)], nrecv.at[k, 0])
        wait_bytes(rb.at[k, 1, pl.ds(0, halves)], nrecv.at[k, 1])
        wait_bytes(rb.at[k, 0, pl.ds(0, halves)], srecv.at[k, 0])
        wait_bytes(rb.at[k, 1, pl.ds(halves, halves)], srecv.at[k, 1])
        whole = yb[k, 0].astype(F32) + rb[k, 0].astype(F32) + rb[k, 1].astype(F32)
        whole = whole.astype(BF)
        laid = jnp.concatenate(
            [whole[:, n * cols : (n + 1) * cols] for n in range(4)], axis=0
        )
        backb[k] = dot(restore, laid).astype(BF)
        for dx, dc in around:
            to = peer((zs - dz) % zs, dx, dc)
            target = to[1] * cs + to[2]
            source = backb.at[k, pl.ds(pl.multiple_of(target * 16, 16), 16)]
            landing = retb.at[k, pl.ds(pl.multiple_of(me * 16, 16), 16)]
            if dz or dx or dc:
                remote(source, landing, bsend.at[k], brecv.at[k], to)
            else:
                landing[...] = source[...]

    def gather_in(k, dz):
        if (spots if dz else spots - 16) > 0:
            wait_bytes(sized(retb, k, dz), brecv.at[k])
        ids = spot_ids((4 * rows, spots), 1, dz)
        share = jnp.where(ids == slot_cols[0], weight_cols[0], 0.0)
        share = share + jnp.where(ids == slot_cols[1], weight_cols[1], 0.0)
        high = share.astype(BF)
        low = (share - high.astype(F32)).astype(BF)
        mix[...] += dot(high, retb[k]) + dot(low, retb[k])

    low, top = pl.ds(0, 2 * rows), pl.ds(2 * rows, 2 * rows)
    wait_bytes(tok.at[1], trecv.at[0])
    remote(tok.at[1, low], tok.at[2, low], tsend.at[2], trecv.at[2], plus)
    wait_bytes(tok.at[3], trecv.at[1])
    remote(tok.at[3, top], tok.at[2, top], tsend.at[3], trecv.at[3], minus)
    mix[...] = tok[0].astype(F32)
    lag_m, lag_b, lag_e, lag_c = LAGS
    for t in range(zs + lag_c):
        if t < len(routed):
            tidy(routed[t])
        if t == 0:
            wait_bytes(tok.at[2, low], trecv.at[2])
            wait_bytes(tok.at[2, top], trecv.at[3])
            for k in direct:
                launch(k)
        if 1 <= t < len(routed) + 1:
            forward(routed[t - 1])
        if lag_m <= t < zs + lag_m:
            feed(t - lag_m)
        if lag_b <= t < zs + lag_b:
            back(t - lag_b, steps[t - lag_b])
        if lag_e <= t < zs + lag_e:
            finish(t - lag_e, steps[t - lag_e])
        if lag_c <= t < zs + lag_c:
            gather_in(t - lag_c, steps[t - lag_c])

    pieces = [mix[n * rows : (n + 1) * rows] for n in range(4)]
    center = sum(jnp.sum(piece, axis=1, keepdims=True) for piece in pieces) / model
    pieces = [piece - center for piece in pieces]
    spread = sum(jnp.sum(piece * piece, axis=1, keepdims=True) for piece in pieces) / model
    scale = lax.rsqrt(spread + eps_layer)
    for n in range(4):
        at = slice(n * cols, (n + 1) * cols)
        out_ref[:, at] = (
            pieces[n] * scale * held["gain"][1:2, at] + held["shift"][1:2, at]
        ).astype(BF)

    if group > 1:
        wait_bytes(buf1.at[pl.ds(0, group - 1)], send1)
    if zs > 1:
        wait_bytes(buf2.at[pl.ds(0, zs - 1)], send2)
    for n in range(6):
        wait_bytes(far.at[0], send3.at[n])
    for n in range(2):
        wait_bytes(tok.at[0], tsend.at[n])
        wait_bytes(tok.at[2, low], tsend.at[n + 2])
    for k, dz in enumerate(steps):
        part = xg.at[k, 0, pl.ds(0, halves)]
        if k in routed:
            wait_bytes(outb.at[k], dsend.at[k])
            for n in range(2):
                wait_bytes(xg.at[k, 0], gsend.at[k, n])
                wait_bytes(part, fsend.at[k, n])
        elif dz or group > 1:
            wait_bytes(sized_q(outq, direct.index(k)), qsend.at[direct.index(k)])
        if dz or group > 1:
            wait_bytes(sized(backb, k, dz), bsend.at[k])
        for n in range(2):
            for sem in (asend, nsend, ssend):
                wait_bytes(part, sem.at[k, n])


def layer(sizes, *args):
    named = dict(zip(NAMES, args))
    wg = args[-3]
    zs, xs, cs, ys = sizes
    length, hk = named["q"].shape
    hv = named["v"].shape[1]
    dv = hv // named["spk"].shape[0]
    rows, model = named["res"].shape
    units = wg.shape[2]
    group = xs * cs
    spots, keep, cols = group * 16, group * 4, model // 4
    dma = pltpu.SemaphoreType.DMA
    hbm = pl.BlockSpec(memory_space=pl.ANY)
    half = rows // 2
    wide = len(plan(zs)[2])
    return pl.pallas_call(
        functools.partial(layer_kernel, sizes),
        out_shape=jax.ShapeDtypeStruct((rows, model), BF),
        in_specs=[hbm] * len(args),
        out_specs=pl.BlockSpec(memory_space=pltpu.VMEM),
        scratch_shapes=[pltpu.VMEM(named[name].shape, named[name].dtype) for name in NAMES]
        + [
            dma((len(NAMES),)),
            pltpu.VMEM((dv + 16, hk), BF),
            pltpu.VMEM((group, dv + 16, hk), BF),
            pltpu.VMEM((dv + 16, hk), BF),
            pltpu.VMEM((zs, dv + 16, hk), BF),
            pltpu.VMEM((len(LEVELS) + 1, length, hk), BF),
            pltpu.VMEM((len(LEVELS) + 1, length, hk), BF),
            pltpu.VMEM((length, hv), F32),
            pltpu.VMEM((length, model), BF),
            pltpu.VMEM((2, half, model), BF),
            pltpu.VMEM((2, 2, half, model), BF),
            pltpu.VMEM((2, half, model), BF),
            dma,
            dma,
            dma,
            dma,
            dma((6,)),
            dma((6,)),
            pltpu.VMEM((model, units), BF),
            pltpu.VMEM((model, units), BF),
            pltpu.VMEM((units, model), BF),
            pltpu.VMEM((4, 4 * rows, cols), BF),
            pltpu.VMEM((4 * rows, cols), F32),
            pltpu.VMEM((zs, spots, cols), BF),
            pltpu.VMEM((zs, spots, cols), BF),
            pltpu.VMEM((wide, 4, spots, cols), BF),
            pltpu.VMEM((wide, 4, spots, cols), BF),
            pltpu.VMEM((zs, ys, keep, model), BF),
            pltpu.VMEM((ys * keep, units), BF),
            pltpu.VMEM((zs, ys, keep, model), BF),
            pltpu.VMEM((zs, 2, keep // 2, model), BF),
            pltpu.VMEM((zs, 2, keep // 2, model), BF),
            pltpu.VMEM((zs, 2, keep, model), BF),
            pltpu.VMEM((zs, spots, cols), BF),
            pltpu.VMEM((zs, spots, cols), BF),
            dma((3,)),
            dma((zs,)),
            dma((zs,)),
        ]
        + [dma((zs, 2))] * 10
        + [dma((zs,)), dma((zs,)), dma((wide,)), dma((wide,)), dma((4,)), dma((4,))],
        compiler_params=pltpu.CompilerParams(
            collective_id=0, has_side_effects=True, vmem_limit_bytes=44 * 1024 * 1024
        ),
        name="layer",
    )(*[pltpu.with_memory_space_constraint(a, pltpu.HBM) for a in args])


def on_device(
    sizes,
    residual,
    queries,
    projected_keys,
    values,
    projected_output_gate,
    decay_gate_input,
    decay_gate_offset,
    decay_spikes,
    documents,
    attention_output_weight,
    layer_norm_gains,
    layer_norm_shifts,
    routes,
    chosen_expert_weights,
    expert_gate_weight,
    expert_up_weight,
    expert_down_weight,
):
    return layer(
        sizes,
        queries,
        projected_keys,
        values,
        projected_output_gate,
        decay_gate_input,
        decay_gate_offset.reshape(1, -1),
        decay_spikes.T,
        documents.reshape(1, -1),
        attention_output_weight,
        residual,
        layer_norm_gains,
        layer_norm_shifts,
        routes.T,
        chosen_expert_weights.T,
        expert_gate_weight,
        expert_up_weight,
        expert_down_weight,
    )


def build(torus):
    sizes = tuple(torus.shape[a] for a in SP_TP)
    return jax.shard_map(
        functools.partial(on_device, sizes),
        mesh=torus,
        in_specs=(
            P(SP_TP, None),
            P(SP, "tp"),
            P(SP, "tp"),
            P(SP, "tp"),
            P(SP, "tp"),
            P(SP, "tp"),
            P("tp"),
            P(SP, "tp"),
            P(SP),
            P("tp", None),
            P(),
            P(),
            P(SP, None),
            P(SP, None),
            P(SP, None, "tp"),
            P(SP, None, "tp"),
            P(SP, "tp", None),
        ),
        out_specs=P(SP_TP, None),
        check_vma=False,
    )


def solution(mesh):
    return build(Mesh(mesh.devices.reshape(8, 4, 2, mesh.shape["tp"]), SP_TP))
```
